32 devices in a mesh: kv: 16 (over z, y, x), tp: 2 (over core).
Axes of the slice: x: 2, y: 2, z: 4, core: 2. Of those that a mesh axis runs over, the one named last changes fastest.
Arguments:
- queries: bfloat16 [14336, 1024], P('kv', 'tp'), may hold values from -6 to 6
- keyvals: bfloat16 [14336, 128], P('kv'), may hold values from -6 to 6
- log_sums: float32 [16, 14336], P('tp', 'kv'), may hold values from 6 to 7.2
- out_grad: bfloat16 [14336, 1024], P('kv', 'tp'), may hold values from -24 to 24
- inputs: bfloat16 [14336, 2048], P('kv'), may hold values from -0.119628906 to 0.119628906
- selection: int32 [112, 16], replicated, may hold values from -1 to 447, as said below
Outputs:
- query_grad: bfloat16 [14336, 1024], P('kv', 'tp')
- keyval_grad: float32 [448, 32, 128], P('kv', 'tp')
- weight_grad: float32 [2048, 1024], P('kv', 'tp')
The draws below stay inside these ranges and needn't reach their ends.
Inputs may be any that keep to these rules, and one draw needn't show every extreme that they name: `selection`: row j first names the key blocks of query block j's own positions in order, then distinct blocks of earlier devices' positions, then -1 entries at the end (only where fewer earlier blocks exist). The rows of one device's query blocks together name at most 2 distinct blocks of any one other device, and exactly 2 for some pair in every draw.
All inputs are finite; a program needn't handle non-finite values.
Results may differ from the reference program's by a relative error of at most 0.0071.
Values may be sent and summed in bfloat16 or wider, within the bound.
A program may use at most 64 MiB of HBM per device.

```python
import jax
import jax.numpy as jnp
from jax import lax

D = 2048
HEADS = 16
DH = 64
QB = 128
KB = 32
NSEL = 16
CAP = 2
TOK_DEV = 896
TOKENS = 14336


def draw_selection(key, part):
    n_dev = TOKENS // TOK_DEV
    own_blocks = TOK_DEV // KB
    per_dev = TOK_DEV // QB
    diagonal = QB // KB
    remote = NSEL - diagonal
    key_elig, key_popular, key_pick = jax.random.split(jax.random.fold_in(key, 7), 3)
    elig_scores = jax.random.randint(key_elig, (n_dev, n_dev, own_blocks), 0, 4096) * own_blocks
    elig_scores = elig_scores + jnp.arange(own_blocks, dtype=jnp.int32)
    unused_values, eligible = lax.top_k(elig_scores, CAP)
    eligible = jnp.arange(n_dev, dtype=jnp.int32)[None, :, None] * own_blocks + eligible.astype(jnp.int32)
    popular = (jax.random.randint(key_popular, (n_dev,), 0, 4) == 0).astype(jnp.int32) * 16384
    picked = jax.random.randint(key_pick, (n_dev, per_dev, n_dev, CAP), 1, 4097)
    device = jnp.arange(n_dev, dtype=jnp.int32)[:, None, None, None]
    owner = jnp.arange(n_dev, dtype=jnp.int32)[None, None, :, None]
    block_row = jnp.arange(per_dev, dtype=jnp.int32)[None, :, None, None]
    slot_col = jnp.arange(CAP, dtype=jnp.int32)[None, None, None, :]
    before = ((owner == device - 1) & (block_row == 0)).astype(jnp.int32)
    halfway = ((owner == device - n_dev // 2) & (block_row == 0) & (slot_col == 0)).astype(jnp.int32)
    wrapped = ((owner == 0) & (device == n_dev - 1) & (block_row == 0) & (slot_col == 0)).astype(jnp.int32)
    score = picked + popular[None, None, :, None] + before * 131072 + halfway * 65536 + wrapped * 32768
    score = jnp.where(owner < device, score, 0)
    composite = (score * (n_dev * CAP) + owner * CAP + slot_col).reshape(n_dev, per_dev, n_dev * CAP)
    top_values, top_index = lax.top_k(composite, remote)
    elig_flat = jnp.broadcast_to(eligible.reshape(n_dev, 1, n_dev * CAP), (n_dev, per_dev, n_dev * CAP))
    chosen = jnp.take_along_axis(elig_flat, top_index.astype(jnp.int32), axis=2)
    chosen = jnp.where(top_values >= n_dev * CAP, chosen, -1)
    diag_ids = (jnp.arange(n_dev, dtype=jnp.int32)[:, None, None] * per_dev + jnp.arange(per_dev, dtype=jnp.int32)[None, :, None]) * diagonal
    diag_ids = diag_ids + jnp.arange(diagonal, dtype=jnp.int32)[None, None, :]
    return jnp.concatenate([diag_ids, chosen], axis=2).reshape(n_dev * per_dev, NSEL).astype(jnp.int32)


def with_spikes(result, stream_key, source, target, shards_of, factor):
    def block_of(dim):
        return (jnp.arange(result.shape[dim]) // (result.shape[dim] // shards_of)).reshape((-1,) + (1,) * (result.ndim - 1 - dim))

    first = jax.random.permutation(stream_key, shards_of)[block_of(target)]
    far = (block_of(target) + shards_of // 2) % shards_of
    return jnp.where((block_of(source) == first) | (block_of(source) == far), factor * result, result)


def level_of(key, shape, cuts, least, high):
    level, own = 1.0, jax.random.fold_in(key, 6)
    for axis_at, blocks in cuts:
        heights = jnp.exp(jax.random.uniform(jax.random.fold_in(own, axis_at), (blocks,), jnp.float32, least / len(cuts), high / len(cuts)))
        level = level * jnp.repeat(heights, shape[axis_at] // blocks).reshape([-1 if axis == axis_at else 1 for axis in range(len(shape))])
    return level


def centred(stream_key, shape, width, limit, cuts=(), held_as=jnp.bfloat16):
    array = width * jax.random.normal(stream_key, shape, jnp.float32)
    if cuts:
        array = array * level_of(stream_key, shape, cuts, -0.22, 0.18)
    return jnp.clip(array, -limit, limit).astype(held_as)


def gaussian_with(rng, shape, width, bound, pieces, heavy, kind=jnp.bfloat16):
    array = width * jax.random.normal(rng, shape, jnp.float32)
    if pieces:
        array = array * level_of(rng, shape, pieces, -0.22, 0.18)
    return jnp.clip(with_spikes(array, jax.random.fold_in(rng, 3), *heavy), -bound, bound).astype(kind)


def setup_inputs(seed: int = 0) -> dict:
    arg_keys = jax.random.split(jax.random.key(seed), 7)
    queries = centred(arg_keys[0], (TOKENS, HEADS * DH), 1.0, 6.0, ((0, 16), (1, 2)))
    keyvals = centred(arg_keys[1], (TOKENS, 2 * DH), 1.0, 6.0, ((0, 16),))
    log_sums = jnp.clip(6.0 + 1.1999998 * jax.random.uniform(arg_keys[2], (HEADS, TOKENS), jnp.float32) ** level_of(arg_keys[2], (HEADS, TOKENS), ((0, 2), (1, 16)), -0.2, 0.2), 6.0, 7.2)
    out_grad = centred(arg_keys[3], (TOKENS, HEADS * DH), 4.0, 24.0, ((0, 16), (1, 2)))
    inputs = gaussian_with(arg_keys[4], (TOKENS, D), 0.02, 0.119628906, ((0, 16),), (0, 1, 16, 2.0))
    selection = draw_selection(jax.random.fold_in(arg_keys[6], 71), 0)
    return {"queries": queries, "keyvals": keyvals, "log_sums": log_sums, "out_grad": out_grad, "inputs": inputs, "selection": selection}


def reference(queries, keyvals, log_sums, out_grad, inputs, selection):
    score_scale = DH ** -0.5
    block_total = TOKENS // KB
    kv_blocks = keyvals.reshape(block_total, KB, 2 * DH)

    def block_step(grad_total, block_index):
        first_row = block_index * QB
        query_rows = lax.dynamic_slice_in_dim(queries, first_row, QB, 0).reshape(QB, HEADS, DH).astype(jnp.float32)
        grad_rows = lax.dynamic_slice_in_dim(out_grad, first_row, QB, 0).reshape(QB, HEADS, DH).astype(jnp.float32)
        log_rows = lax.dynamic_slice_in_dim(log_sums, first_row, QB, 1)
        block_list = lax.dynamic_index_in_dim(selection, block_index, 0, keepdims=False)
        safe_list = jnp.maximum(block_list, 0).astype(jnp.int32)
        chosen = jnp.take(kv_blocks, safe_list, axis=0).reshape(NSEL * KB, 2 * DH).astype(jnp.float32)
        key_rows = chosen[:, :DH]
        value_rows = chosen[:, DH:]
        key_pos = (safe_list[:, None] * KB + jnp.arange(KB, dtype=jnp.int32)[None, :]).reshape(-1)
        key_live = jnp.repeat(block_list >= 0, KB)
        query_pos = first_row + jnp.arange(QB, dtype=jnp.int32)
        live_mask = key_live[None, :] & (key_pos[None, :] <= query_pos[:, None])
        scores = jnp.einsum("thd,kd->htk", query_rows, key_rows) * score_scale
        prob_f32 = jnp.where(live_mask[None], jnp.exp(scores - log_rows[:, :, None]), 0.0)
        prob_b = prob_f32.astype(jnp.bfloat16).astype(jnp.float32)
        recomputed = jnp.einsum("htk,kd->thd", prob_b, value_rows)
        row_delta = jnp.sum(grad_rows * recomputed, axis=-1)
        dprob = jnp.einsum("thd,kd->htk", grad_rows, value_rows)
        dscore = prob_f32 * (dprob - jnp.transpose(row_delta)[:, :, None])
        dscore_b = dscore.astype(jnp.bfloat16).astype(jnp.float32)
        query_grad = (jnp.einsum("htk,kd->thd", dscore_b, key_rows) * score_scale).astype(jnp.bfloat16)
        key_grad = jnp.einsum("htk,thd->kd", dscore_b, query_rows) * score_scale
        value_grad = jnp.einsum("htk,thd->kd", prob_b, grad_rows)
        entry_grads = jnp.concatenate([key_grad, value_grad], axis=-1).reshape(NSEL, KB, 2 * DH)
        grad_total = grad_total.at[safe_list].add(entry_grads)
        return grad_total, query_grad.reshape(QB, HEADS * DH)

    start_total = jnp.zeros((block_total, KB, 2 * DH), jnp.float32)
    keyval_grad, query_blocks = lax.scan(block_step, start_total, jnp.arange(TOKENS // QB, dtype=jnp.int32))
    query_grad = query_blocks.reshape(TOKENS, HEADS * DH)
    weight_grad = lax.dot_general(inputs, query_grad, (((0,), (0,)), ((), ())), preferred_element_type=jnp.float32)
    return query_grad, keyval_grad, weight_grad
```

```python
import functools

import jax
import jax.numpy as jnp
from jax import lax
from jax.experimental import pallas as pl
from jax.experimental.pallas import tpu as pltpu
from jax.sharding import PartitionSpec as P

DH = 64
QB = 128
KB = 32
NSEL = 16
CAP = 2
LOG2E = 1.4426950408889634
DEAD = 1e30
GROUP = 1
UNROLL = True
VMEM_LIMIT = 28 * 1024 * 1024
MESH = pl.DeviceIdType.MESH


def slot_table(wanted):
    slot_rank = jnp.cumsum(wanted.astype(jnp.int32), axis=1) - 1
    return wanted[:, None, :] & (
        slot_rank[:, None, :] == jnp.arange(CAP, dtype=jnp.int32)[None, :, None]
    )


def weight_term(inputs, query_grad):
    return lax.dot_general(
        inputs, query_grad, (((0,), (0,)), ((), ())), preferred_element_type=jnp.float32
    )


def body(queries, keyvals, log_sums, out_grad, inputs, selection):
    kv_count = lax.axis_size("kv")
    own_index = lax.axis_index("kv")
    tok_count, width = queries.shape
    head_count = width // DH
    per_dev = tok_count // QB
    own_blocks = tok_count // KB
    slot_count = kv_count * CAP
    score_scale = DH ** (-0.5)
    own_kv = keyvals.reshape(own_blocks, KB, 2 * DH)
    lists = selection.reshape(kv_count, per_dev * NSEL)
    device_ids = jnp.arange(kv_count, dtype=jnp.int32)
    mine = own_index * own_blocks + jnp.arange(own_blocks, dtype=jnp.int32)
    wanted = jnp.any(lists[:, :, None] == mine[None, None, :], axis=1) & (
        device_ids[:, None] != own_index
    )
    owner_slots = slot_table(wanted)
    outgoing = jnp.einsum(
        "rsb,bkc->rskc",
        owner_slots.astype(jnp.bfloat16),
        own_kv,
        preferred_element_type=jnp.float32,
    ).astype(jnp.bfloat16)
    fetched = lax.all_to_all(outgoing, "kv", split_axis=0, concat_axis=0, tiled=True)
    block_list = lax.dynamic_index_in_dim(lists, own_index, 0, keepdims=False)
    every_block = jnp.arange(kv_count * own_blocks, dtype=jnp.int32)
    hits = block_list[:, None] == every_block[None, :]
    needed = jnp.any(hits, axis=0).reshape(kv_count, own_blocks) & (
        device_ids[:, None] != own_index
    )
    slot_rank = jnp.cumsum(needed.astype(jnp.int32), axis=1) - 1
    entry_rank = jnp.sum(jnp.where(hits, slot_rank.reshape(-1)[None, :], 0), axis=1)
    safe_list = jnp.maximum(block_list, 0)
    owner_index = safe_list // own_blocks
    local_block = safe_list % own_blocks
    pool_index = jnp.where(
        owner_index == own_index, slot_count + local_block, owner_index * CAP + entry_rank
    )
    pool_index = jnp.where(block_list < 0, 0, pool_index)
    block_pool = jnp.concatenate([fetched.reshape(slot_count, KB, 2 * DH), own_kv], axis=0)
    gathered = jnp.take(block_pool, pool_index, axis=0).reshape(per_dev, NSEL * KB, 2 * DH)
    key_rows = gathered[:, :, :DH]
    value_rows = gathered[:, :, DH:]
    query_rows = queries.reshape(per_dev, QB, head_count, DH)
    grad_rows = out_grad.reshape(per_dev, QB, head_count, DH)
    log_rows = log_sums.reshape(head_count, per_dev, QB).transpose(1, 0, 2)
    key_pos = (
        safe_list.reshape(per_dev, NSEL, 1) * KB + jnp.arange(KB, dtype=jnp.int32)[None, None, :]
    ).reshape(per_dev, NSEL * KB)
    key_live = jnp.repeat((block_list >= 0).reshape(per_dev, NSEL), KB, axis=1)
    query_pos = own_index * tok_count + jnp.arange(tok_count, dtype=jnp.int32).reshape(per_dev, QB)
    live_mask = key_live[:, None, :] & (key_pos[:, None, :] <= query_pos[:, :, None])
    scores = (
        jnp.einsum("pthd,pkd->phtk", query_rows, key_rows, preferred_element_type=jnp.float32)
        * score_scale
    )
    prob_f32 = jnp.where(live_mask[:, None], jnp.exp(scores - log_rows[..., None]), 0.0)
    prob_b = prob_f32.astype(jnp.bfloat16)
    recomputed = jnp.einsum(
        "phtk,pkd->pthd", prob_b, value_rows, preferred_element_type=jnp.float32
    )
    row_delta = jnp.sum(grad_rows.astype(jnp.float32) * recomputed, axis=-1)
    dprob = jnp.einsum("pthd,pkd->phtk", grad_rows, value_rows, preferred_element_type=jnp.float32)
    dscore = prob_f32 * (dprob - row_delta.transpose(0, 2, 1)[..., None])
    dscore_b = dscore.astype(jnp.bfloat16)
    query_grad = (
        (
            jnp.einsum("phtk,pkd->pthd", dscore_b, key_rows, preferred_element_type=jnp.float32)
            * score_scale
        )
        .astype(jnp.bfloat16)
        .reshape(tok_count, width)
    )
    key_grad = (
        jnp.einsum("phtk,pthd->pkd", dscore_b, query_rows, preferred_element_type=jnp.float32)
        * score_scale
    )
    value_grad = jnp.einsum("phtk,pthd->pkd", prob_b, grad_rows, preferred_element_type=jnp.float32)
    entry_grads = jnp.concatenate([key_grad, value_grad], axis=-1).reshape(
        per_dev * NSEL, KB, 2 * DH
    )
    spread = (
        pool_index[:, None] == jnp.arange(slot_count + own_blocks, dtype=jnp.int32)[None, :]
    ).astype(jnp.float32)
    shares = lax.psum_scatter(entry_grads, "tp", scatter_dimension=1, tiled=True)
    summed = jnp.einsum("ep,ekc->pkc", spread, shares, precision=lax.Precision.HIGHEST)
    key_share = summed.shape[1]
    returned = lax.all_to_all(
        summed[:slot_count].reshape(kv_count, CAP, key_share, 2 * DH).astype(jnp.bfloat16),
        "kv",
        split_axis=0,
        concat_axis=0,
        tiled=True,
    ).astype(jnp.float32)
    keyval_grad = (
        jnp.einsum(
            "rsb,rskc->bkc",
            owner_slots.astype(jnp.float32),
            returned,
            precision=lax.Precision.HIGHEST,
        )
        + summed[slot_count:]
    )
    weight_grad = lax.psum_scatter(
        weight_term(inputs, query_grad), "kv", scatter_dimension=0, tiled=True
    )
    return (query_grad, keyval_grad, weight_grad)


def bit_orders(kv_count, chunk_count):
    bits = kv_count.bit_length() - 1
    orders = []
    for c in range(chunk_count):
        turn = c % 3
        first = [0, 1, 2]
        orders.append(first[turn:] + first[:turn] + list(range(3, bits)))
    return orders


def flip(index, place):
    bit = (index // (1 << place)) % 2
    return index + (1 - 2 * bit) * (1 << place)


def fused_kernel(
    kv_count,
    orders,
    sel_hbm,
    own_hbm,
    log_hbm,
    q_hbm,
    g_hbm,
    in_hbm,
    qg_ref,
    wg_ref,
    kvg_ref,
    sel_scr,
    first_scr,
    table_scr,
    first_ref,
    table_ref,
    out_scr,
    log_ref,
    own_scr,
    q_scr,
    g_scr,
    in_scr,
    pool_scr,
    kv_scr,
    kt_scr,
    dkv_scr,
    qgt_scr,
    total,
    half_scr,
    tp_scr,
    slot_scr,
    ret_scr,
    *rest,
):
    bits = len(orders[0])
    chunk_count = len(orders)
    send_scr = rest[:bits]
    recv_scr = rest[bits : 2 * bits]
    load_sem, get_send, get_recv, tp_send, tp_recv, ret_send, ret_recv, w_send, w_recv = rest[2 * bits :]
    me = lax.axis_index("kv")
    core = lax.axis_index("tp")
    other = 1 - core
    rows, width = wg_ref.shape
    pair_count = width // (2 * DH * GROUP)
    per_dev = q_scr.shape[0] // QB
    slot_count = kv_count * CAP
    entry_count = per_dev * NSEL
    diagonal = QB // KB
    half = KB // 2
    score_scale = DH ** (-0.5)

    def peer(step):
        return lax.rem(me + step, kv_count)

    own_blocks = own_hbm.shape[0]
    loads = [
        pltpu.make_async_copy(src, dst, load_sem.at[i])
        for i, (src, dst) in enumerate(
            (
                (sel_hbm, sel_scr),
                (own_hbm, own_scr),
                (log_hbm, log_ref),
                (q_hbm, q_scr),
                (g_hbm, g_scr),
                (in_hbm, in_scr),
                (first_scr, first_ref),
                (table_scr, table_ref),
            )
        )
    ]
    for load in loads[:6]:
        load.start()
    pool_scr[...] = jnp.zeros(pool_scr.shape, jnp.bfloat16)
    ret_scr[...] = jnp.zeros(ret_scr.shape, jnp.bfloat16)

    barrier = pltpu.get_barrier_semaphore()
    for step in range(1, kv_count):
        pl.semaphore_signal(barrier, inc=1, device_id=(peer(step), core), device_id_type=MESH)
    pl.semaphore_signal(barrier, inc=1, device_id=(me, other), device_id_type=MESH)

    loads[0].wait()
    chosen = padded(sel_scr[...])
    first_scr[...] = first_table(chosen, me * own_blocks, own_blocks, per_dev)
    loads[6].start()
    table_scr[...] = entry_table(chosen, me, kv_count, own_blocks, per_dev)
    loads[7].start()
    dkv_scr[entry_count] = jnp.zeros((KB, 2 * DH), jnp.float32)
    loads[1].wait()
    loads[6].wait()
    for r in range(kv_count):
        for s in range(CAP):
            out_scr[r, s] = own_scr[first_ref[s, r * per_dev]]
    pl.semaphore_wait(barrier, kv_count)

    def get_copy(target, source):
        return pltpu.make_async_remote_copy(
            src_ref=out_scr.at[target],
            dst_ref=pool_scr.at[pl.ds(source * CAP, CAP)],
            send_sem=get_send.at[target],
            recv_sem=get_recv.at[source],
            device_id=(target, core),
            device_id_type=MESH,
        )

    def later(do):
        for step in range(kv_count - 1, 0, -1):
            @pl.when(me + step < kv_count)
            def _():
                do(me + step)

    def earlier(do):
        for step in range(1, kv_count):
            @pl.when(me >= step)
            def _():
                do(me - step)

    later(lambda r: get_copy(r, me).start())
    for load in loads[2:5]:
        load.wait()
    loads[7].wait()
    earlier(lambda r: get_copy(me, r).wait_recv())

    def gather(p, carry):
        for e in range(diagonal):
            kv_scr[p, e * KB : (e + 1) * KB, :] = own_scr[p * diagonal + e]
        for e in range(diagonal, NSEL):
            kv_scr[p, e * KB : (e + 1) * KB, :] = pool_scr[table_ref[e, p]]
        kt_scr[p] = kv_scr[p][:, :DH].T
        return carry

    lax.fori_loop(0, per_dev, gather, 0)

    key_row = lax.broadcasted_iota(jnp.int32, (QB, 2 * QB), 0)
    query_col = lax.broadcasted_iota(jnp.int32, (QB, 2 * QB), 1) % QB
    causal = key_row <= query_col
    nt = (((1,), (1,)), ((), ()))

    def attend(group):
        def block(p, carry):
            tok = pl.ds(pl.multiple_of(p * QB, QB), QB)
            keys = kv_scr[p, :, :DH]
            values = kv_scr[p, :, DH:]
            penalty = [
                jnp.where(table_ref[NSEL + e, p] >= 0, jnp.float32(0.0), jnp.float32(DEAD))
                for e in range(NSEL)
            ]
            dkv = None
            for pair in range(group * GROUP, (group + 1) * GROUP):
                at = pair * 2 * DH
                q2 = jnp.concatenate([q_scr[tok, at : at + DH], q_scr[tok, at + DH : at + 2 * DH]], axis=0)
                g2 = jnp.concatenate([g_scr[tok, at : at + DH], g_scr[tok, at + DH : at + 2 * DH]], axis=0)
                log2 = jnp.concatenate(
                    [log_ref[2 * pair : 2 * pair + 1, tok], log_ref[2 * pair + 1 : 2 * pair + 2, tok]], axis=1
                )
                log2 = log2 * LOG2E
                scores = lax.dot_general(keys, q2, nt, preferred_element_type=jnp.float32)
                dprob = lax.dot_general(values, g2, nt, preferred_element_type=jnp.float32)
                shifted = jnp.concatenate(
                    [
                        scores[e * KB : (e + 1) * KB] * (score_scale * LOG2E) - (log2 + penalty[e])
                        for e in range(NSEL)
                    ],
                    axis=0,
                )
                shifted = jnp.concatenate([jnp.where(causal, shifted[:QB], -DEAD), shifted[QB:]], axis=0)
                prob = jnp.exp2(shifted)
                prob_b = prob.astype(jnp.bfloat16)
                delta = jnp.sum(prob_b.astype(jnp.float32) * dprob, axis=0, keepdims=True)
                dscore_b = (prob * (dprob - delta)).astype(jnp.bfloat16)
                dq = jnp.dot(kt_scr[p], dscore_b, preferred_element_type=jnp.float32) * score_scale
                dq = jnp.concatenate([dq[:, :QB], dq[:, QB:]], axis=0)
                qgt_scr[at : at + 2 * DH, tok] = dq.astype(jnp.bfloat16)
                qg_ref[tok, at : at + 2 * DH] = dq.T.astype(jnp.bfloat16)
                dk = jnp.dot(dscore_b, q2, preferred_element_type=jnp.float32) * score_scale
                dv = jnp.dot(prob_b, g2, preferred_element_type=jnp.float32)
                part = jnp.concatenate([dk, dv], axis=1)
                dkv = part if dkv is None else dkv + part
            dkv = dkv.reshape(NSEL, KB, 2 * DH)
            entries = pl.ds(p * NSEL, NSEL)
            if group > 0:
                dkv = dkv + dkv_scr[entries]
            dkv_scr[entries] = dkv
            return carry

        lax.fori_loop(0, per_dev, block, 0, unroll=UNROLL)

    def product(pair):
        cols = slice(pair * GROUP * 2 * DH, (pair + 1) * GROUP * 2 * DH)

        def piece(j, carry):
            at = pl.multiple_of(j * 2 * rows, 2 * rows)
            part = jnp.dot(
                qgt_scr[cols, :], in_scr[:, pl.ds(at, 2 * rows)], preferred_element_type=jnp.float32
            )
            total[2 * j, cols, :] = part[:, :rows]
            total[2 * j + 1, cols, :] = part[:, rows:]
            return carry

        lax.fori_loop(0, kv_count // 2, piece, 0)

    def owner_of(c, slot):
        owner = me
        for k in range(bits):
            if (slot >> (bits - 1 - k)) & 1:
                owner = flip(owner, orders[c][k])
        return owner

    def current(c, slot, k):
        at = owner_of(c, slot)
        value = total[at, c * DH : (c + 1) * DH, :]
        if k > 0:
            value = value + recv_scr[k - 1][c, slot].astype(jnp.float32)
            total[at, c * DH : (c + 1) * DH, :] = value
        return value

    def weight_copy(c, k):
        return pltpu.make_async_remote_copy(
            src_ref=send_scr[k].at[c],
            dst_ref=recv_scr[k].at[c],
            send_sem=w_send.at[c, k],
            recv_sem=w_recv.at[c, k],
            device_id=(flip(me, orders[c][k]), core),
            device_id_type=MESH,
        )

    def weight_stage(pair, k):
        left = kv_count >> (k + 1)
        for c in range(2 * GROUP * pair, 2 * GROUP * (pair + 1)):
            if k > 0:
                weight_copy(c, k - 1).wait_recv()
            if k == bits:
                value = total[me, c * DH : (c + 1) * DH, :] + recv_scr[k - 1][c, 0].astype(jnp.float32)
                wg_ref[:, c * DH : (c + 1) * DH] = value.T
                continue
            for slot in range(left, 2 * left):
                send_scr[k][c, slot - left] = current(c, slot, k).astype(jnp.bfloat16)
            weight_copy(c, k).start()
            if k > 0:
                for slot in range(left):
                    current(c, slot, k)

    def advance(turn):
        for k in range(bits + 1):
            if 0 <= turn - k < pair_count:
                weight_stage(turn - k, k)

    tp_copy = pltpu.make_async_remote_copy(
        src_ref=half_scr.at[other],
        dst_ref=tp_scr,
        send_sem=tp_send,
        recv_sem=tp_recv,
        device_id=(me, other),
        device_id_type=MESH,
    )

    def ret_copy(target, source):
        return pltpu.make_async_remote_copy(
            src_ref=slot_scr.at[target],
            dst_ref=ret_scr.at[source],
            send_sem=ret_send.at[target],
            recv_sem=ret_recv.at[source],
            device_id=(target, core),
            device_id_type=MESH,
        )

    def collect(s, carry):
        value = dkv_scr[table_ref[2 * NSEL + s, 0]]
        for p in range(1, per_dev):
            value = value + dkv_scr[table_ref[2 * NSEL + s, p]]
        half_scr[0, s] = value[:half]
        half_scr[1, s] = value[half:]
        return carry

    for pair in range(pair_count):
        attend(pair)
        if pair == 0:
            loads[5].wait()
        if pair == pair_count - 1:
            lax.fori_loop(0, slot_count, collect, 0)
            for p in range(per_dev):
                at = slot_count + p * diagonal
                half_scr[0, at : at + diagonal] = dkv_scr[p * NSEL : p * NSEL + diagonal, :half, :]
                half_scr[1, at : at + diagonal] = dkv_scr[p * NSEL : p * NSEL + diagonal, half:, :]
            tp_copy.start()
        product(pair)
        advance(pair)

    tp_copy.wait_recv()
    mine = half_scr.at[core]
    slot_scr[...] = (
        (mine[:slot_count] + tp_scr[:slot_count])
        .astype(jnp.bfloat16)
        .reshape(kv_count, CAP, half, 2 * DH)
    )
    earlier(lambda r: ret_copy(r, me).start())
    own_sum = (mine[slot_count:] + tp_scr[slot_count:]).reshape(own_blocks * half, 2 * DH)

    for turn in range(pair_count, pair_count + bits):
        advance(turn)
    later(lambda r: ret_copy(me, r).wait_recv())
    column = lax.broadcasted_iota(jnp.int32, (1, slot_count * half), 1)
    block = jnp.zeros(column.shape, jnp.int32)
    for r in range(kv_count):
        for s in range(CAP):
            block = jnp.where(column // half == r * CAP + s, first_ref[s, r * per_dev], block)
    wanted = block * half + column % half
    row = lax.broadcasted_iota(jnp.int32, (own_blocks * half, slot_count * half), 0)
    spread = jnp.where(row == wanted, 1.0, 0.0).astype(jnp.bfloat16)
    back = ret_scr[...].reshape(slot_count * half, 2 * DH)
    kvg = own_sum + jnp.dot(spread, back, preferred_element_type=jnp.float32)
    kvg_ref[...] = kvg.reshape(own_blocks, half, 2 * DH)
    later(lambda r: get_copy(r, me).wait_send())
    earlier(lambda r: ret_copy(r, me).wait_send())
    tp_copy.wait_send()
    for c in range(chunk_count):
        for k in range(bits):
            weight_copy(c, k).wait_send()


def padded(chosen):
    fill = jnp.full((NSEL, 128 - chosen.shape[1]), -1, jnp.int32)
    return jnp.concatenate([chosen, fill], axis=1)


def first_table(chosen, base, own_blocks, per_dev):
    inside = (chosen >= base) & (chosen < base + own_blocks)
    low = jnp.min(jnp.where(inside, chosen - base, own_blocks), axis=0, keepdims=True)
    high = jnp.max(jnp.where(inside, chosen - base, -1), axis=0, keepdims=True)
    cover = 1
    while cover < per_dev:
        shift = 128 - min(cover, per_dev - cover)
        low = jnp.minimum(low, pltpu.roll(low, shift, 1))
        high = jnp.maximum(high, pltpu.roll(high, shift, 1))
        cover = min(2 * cover, per_dev)
    low = jnp.where(low == own_blocks, 0, low)
    high = jnp.maximum(high, 0)
    row = lax.broadcasted_iota(jnp.int32, (8, 128), 0)
    return jnp.where(row == 0, low, high)


def entry_table(chosen, me, kv_count, own_blocks, per_dev):
    slot_count = kv_count * CAP
    spare = per_dev * NSEL
    lane = lax.broadcasted_iota(jnp.int32, (NSEL, 128), 1)
    entry = lax.broadcasted_iota(jnp.int32, (NSEL, 128), 0) + lane * NSEL
    blocks = pltpu.roll(chosen, lax.rem(128 - me * per_dev + 128, 128), 1)
    blocks = jnp.where(lane < per_dev, blocks, -1)
    top = kv_count * own_blocks
    lows = []
    for o in range(kv_count):
        inside = (blocks >= o * own_blocks) & (blocks < (o + 1) * own_blocks)
        lows.append(jnp.min(jnp.where(inside, blocks, top), axis=0, keepdims=True))
    low = jnp.min(jnp.concatenate(lows, axis=0), axis=1, keepdims=True)
    slot = jnp.full((NSEL, 128), slot_count, jnp.int32)
    for o in range(kv_count):
        inside = (blocks >= o * own_blocks) & (blocks < (o + 1) * own_blocks)
        at = o * CAP + jnp.where(blocks > low[o : o + 1], 1, 0)
        slot = jnp.where(inside, at, slot)
    mine = (blocks >= me * own_blocks) & (blocks < (me + 1) * own_blocks)
    slot = jnp.where(mine, slot_count, slot)
    places = []
    for s in range(slot_count):
        found = jnp.max(jnp.where(slot == s, entry, -1), axis=0, keepdims=True)
        places.append(jnp.where(found < 0, spare, found))
    return jnp.concatenate([jnp.minimum(slot, slot_count - 1), blocks] + places, axis=0)


def finish_kernel(qg_ref, wg_ref, kvg_ref, qg_out, wg_out, kvg_out, sem):
    pairs = ((qg_ref, qg_out), (wg_ref, wg_out), (kvg_ref, kvg_out))
    copies = [pltpu.make_async_copy(src, dst, sem.at[i]) for i, (src, dst) in enumerate(pairs)]
    for copy in copies:
        copy.start()
    for copy in copies:
        copy.wait()


def finish(*results):
    hbm = pl.BlockSpec(memory_space=pl.ANY)
    return pl.pallas_call(
        finish_kernel,
        out_shape=[jax.ShapeDtypeStruct(r.shape, r.dtype) for r in results],
        in_specs=[hbm] * 3,
        out_specs=[hbm] * 3,
        scratch_shapes=[pltpu.SemaphoreType.DMA((3,))],
        compiler_params=pltpu.CompilerParams(vmem_limit_bytes=1024 * 1024),
        name="finish",
    )(*results)


def fused(kv_count, chosen, own_kv, log_sums, queries, out_grad, inputs):
    operands = (chosen, own_kv, log_sums, queries, out_grad, inputs)
    tok_count, width = queries.shape
    per_dev = tok_count // QB
    rows = inputs.shape[1] // kv_count
    chunk_count = width // DH
    orders = bit_orders(kv_count, chunk_count)
    bits = len(orders[0])
    slot_count = kv_count * CAP
    pool_count = slot_count + own_kv.shape[0]
    half = KB // 2
    parts = [
        pltpu.VMEM((chunk_count, kv_count >> (k + 1), DH, rows), jnp.bfloat16) for k in range(bits)
    ]
    vmem = pl.BlockSpec(memory_space=pltpu.VMEM)
    hbm = pl.BlockSpec(memory_space=pl.ANY)
    dma = pltpu.SemaphoreType.DMA
    table_rows = 2 * NSEL + slot_count
    return pl.pallas_call(
        functools.partial(fused_kernel, kv_count, orders),
        out_shape=[
            pltpu.VMEM((tok_count, width), jnp.bfloat16),
            pltpu.VMEM((rows, width), jnp.float32),
            pltpu.VMEM((own_kv.shape[0], half, 2 * DH), jnp.float32),
        ],
        in_specs=[hbm] * 6,
        out_specs=[vmem] * 3,
        scratch_shapes=[
            pltpu.VMEM(chosen.shape, jnp.int32),
            pltpu.VMEM((8, 128), jnp.int32),
            pltpu.VMEM((table_rows, 128), jnp.int32),
            pltpu.SMEM((8, 128), jnp.int32),
            pltpu.SMEM((table_rows, 128), jnp.int32),
            pltpu.VMEM((kv_count, CAP, KB, 2 * DH), jnp.bfloat16),
            pltpu.VMEM(log_sums.shape, jnp.float32),
            pltpu.VMEM(own_kv.shape, jnp.bfloat16),
            pltpu.VMEM((tok_count, width), jnp.bfloat16),
            pltpu.VMEM((tok_count, width), jnp.bfloat16),
            pltpu.VMEM(inputs.shape, jnp.bfloat16),
            pltpu.VMEM((slot_count, KB, 2 * DH), jnp.bfloat16),
            pltpu.VMEM((per_dev, NSEL * KB, 2 * DH), jnp.bfloat16),
            pltpu.VMEM((per_dev, DH, NSEL * KB), jnp.bfloat16),
            pltpu.VMEM((per_dev * NSEL + 1, KB, 2 * DH), jnp.float32),
            pltpu.VMEM((width, tok_count), jnp.bfloat16),
            pltpu.VMEM((kv_count, width, rows), jnp.float32),
            pltpu.VMEM((2, pool_count, half, 2 * DH), jnp.float32),
            pltpu.VMEM((pool_count, half, 2 * DH), jnp.float32),
            pltpu.VMEM((kv_count, CAP, half, 2 * DH), jnp.bfloat16),
            pltpu.VMEM((kv_count, CAP, half, 2 * DH), jnp.bfloat16),
        ]
        + parts
        + parts
        + [
            dma((8,)),
            dma((kv_count,)),
            dma((kv_count,)),
            dma,
            dma,
            dma((kv_count,)),
            dma((kv_count,)),
            dma((chunk_count, bits)),
            dma((chunk_count, bits)),
        ],
        compiler_params=pltpu.CompilerParams(
            collective_id=0, has_side_effects=True, vmem_limit_bytes=VMEM_LIMIT
        ),
        name="fused",
    )(*(pltpu.with_memory_space_constraint(x, pltpu.HBM) for x in operands))


def fused_body(queries, keyvals, log_sums, out_grad, inputs, selection):
    kv_count = lax.axis_size("kv")
    own_blocks = queries.shape[0] // KB
    own_kv = keyvals.reshape(own_blocks, KB, 2 * DH)
    results = fused(kv_count, selection.T, own_kv, log_sums, queries, out_grad, inputs)
    query_grad, weight_grad, keyval_grad = finish(*results)
    return (query_grad, keyval_grad, weight_grad)


def fits(kv_count, tp_count, tok_count, rows, width):
    power = kv_count & (kv_count - 1) == 0 and kv_count >= 8
    lanes = power and kv_count <= NSEL and kv_count * (tok_count // QB) <= 128
    return tp_count == 2 and lanes and rows % 128 == 0 and width % (2 * DH * GROUP) == 0


def step(queries, keyvals, log_sums, out_grad, inputs, selection):
    kv_count, tp_count = lax.axis_size("kv"), lax.axis_size("tp")
    chosen = fits(kv_count, tp_count, queries.shape[0], inputs.shape[1] // kv_count, queries.shape[1])
    return (fused_body if chosen else body)(
        queries, keyvals, log_sums, out_grad, inputs, selection
    )


def solution(mesh):
    return jax.shard_map(
        step,
        mesh=mesh,
        in_specs=(P("kv", "tp"), P("kv", None), P("tp", "kv"), P("kv", "tp"), P("kv", None), P()),
        out_specs=(P("kv", "tp"), P("kv", "tp", None), P("kv", "tp")),
        check_vma=False,
    )
```

```python
import functools

import jax
import jax.numpy as jnp
from jax import lax
from jax.experimental import pallas as pl
from jax.experimental.pallas import tpu as pltpu
from jax.sharding import PartitionSpec as P

DH = 64
QB = 128
KB = 32
NSEL = 16
CAP = 2
LOG2E = 1.4426950408889634
DEAD = 1e30
GROUP = 1
UNROLL = True
PIECES = 8
KEYS = 7
VMEM_LIMIT = 48 * 1024 * 1024
MESH = pl.DeviceIdType.MESH


def slot_table(wanted):
    slot_rank = jnp.cumsum(wanted.astype(jnp.int32), axis=1) - 1
    return wanted[:, None, :] & (
        slot_rank[:, None, :] == jnp.arange(CAP, dtype=jnp.int32)[None, :, None]
    )


def weight_term(inputs, query_grad):
    return lax.dot_general(
        inputs, query_grad, (((0,), (0,)), ((), ())), preferred_element_type=jnp.float32
    )


def body(queries, keyvals, log_sums, out_grad, inputs, selection):
    kv_count = lax.axis_size("kv")
    own_index = lax.axis_index("kv")
    tok_count, width = queries.shape
    head_count = width // DH
    per_dev = tok_count // QB
    own_blocks = tok_count // KB
    slot_count = kv_count * CAP
    score_scale = DH ** (-0.5)
    own_kv = keyvals.reshape(own_blocks, KB, 2 * DH)
    lists = selection.reshape(kv_count, per_dev * NSEL)
    device_ids = jnp.arange(kv_count, dtype=jnp.int32)
    mine = own_index * own_blocks + jnp.arange(own_blocks, dtype=jnp.int32)
    wanted = jnp.any(lists[:, :, None] == mine[None, None, :], axis=1) & (
        device_ids[:, None] != own_index
    )
    owner_slots = slot_table(wanted)
    outgoing = jnp.einsum(
        "rsb,bkc->rskc",
        owner_slots.astype(jnp.bfloat16),
        own_kv,
        preferred_element_type=jnp.float32,
    ).astype(jnp.bfloat16)
    fetched = lax.all_to_all(outgoing, "kv", split_axis=0, concat_axis=0, tiled=True)
    block_list = lax.dynamic_index_in_dim(lists, own_index, 0, keepdims=False)
    every_block = jnp.arange(kv_count * own_blocks, dtype=jnp.int32)
    hits = block_list[:, None] == every_block[None, :]
    needed = jnp.any(hits, axis=0).reshape(kv_count, own_blocks) & (
        device_ids[:, None] != own_index
    )
    slot_rank = jnp.cumsum(needed.astype(jnp.int32), axis=1) - 1
    entry_rank = jnp.sum(jnp.where(hits, slot_rank.reshape(-1)[None, :], 0), axis=1)
    safe_list = jnp.maximum(block_list, 0)
    owner_index = safe_list // own_blocks
    local_block = safe_list % own_blocks
    pool_index = jnp.where(
        owner_index == own_index, slot_count + local_block, owner_index * CAP + entry_rank
    )
    pool_index = jnp.where(block_list < 0, 0, pool_index)
    block_pool = jnp.concatenate([fetched.reshape(slot_count, KB, 2 * DH), own_kv], axis=0)
    gathered = jnp.take(block_pool, pool_index, axis=0).reshape(per_dev, NSEL * KB, 2 * DH)
    key_rows = gathered[:, :, :DH]
    value_rows = gathered[:, :, DH:]
    query_rows = queries.reshape(per_dev, QB, head_count, DH)
    grad_rows = out_grad.reshape(per_dev, QB, head_count, DH)
    log_rows = log_sums.reshape(head_count, per_dev, QB).transpose(1, 0, 2)
    key_pos = (
        safe_list.reshape(per_dev, NSEL, 1) * KB + jnp.arange(KB, dtype=jnp.int32)[None, None, :]
    ).reshape(per_dev, NSEL * KB)
    key_live = jnp.repeat((block_list >= 0).reshape(per_dev, NSEL), KB, axis=1)
    query_pos = own_index * tok_count + jnp.arange(tok_count, dtype=jnp.int32).reshape(per_dev, QB)
    live_mask = key_live[:, None, :] & (key_pos[:, None, :] <= query_pos[:, :, None])
    scores = (
        jnp.einsum("pthd,pkd->phtk", query_rows, key_rows, preferred_element_type=jnp.float32)
        * score_scale
    )
    prob_f32 = jnp.where(live_mask[:, None], jnp.exp(scores - log_rows[..., None]), 0.0)
    prob_b = prob_f32.astype(jnp.bfloat16)
    recomputed = jnp.einsum(
        "phtk,pkd->pthd", prob_b, value_rows, preferred_element_type=jnp.float32
    )
    row_delta = jnp.sum(grad_rows.astype(jnp.float32) * recomputed, axis=-1)
    dprob = jnp.einsum("pthd,pkd->phtk", grad_rows, value_rows, preferred_element_type=jnp.float32)
    dscore = prob_f32 * (dprob - row_delta.transpose(0, 2, 1)[..., None])
    dscore_b = dscore.astype(jnp.bfloat16)
    query_grad = (
        (
            jnp.einsum("phtk,pkd->pthd", dscore_b, key_rows, preferred_element_type=jnp.float32)
            * score_scale
        )
        .astype(jnp.bfloat16)
        .reshape(tok_count, width)
    )
    key_grad = (
        jnp.einsum("phtk,pthd->pkd", dscore_b, query_rows, preferred_element_type=jnp.float32)
        * score_scale
    )
    value_grad = jnp.einsum("phtk,pthd->pkd", prob_b, grad_rows, preferred_element_type=jnp.float32)
    entry_grads = jnp.concatenate([key_grad, value_grad], axis=-1).reshape(
        per_dev * NSEL, KB, 2 * DH
    )
    spread = (
        pool_index[:, None] == jnp.arange(slot_count + own_blocks, dtype=jnp.int32)[None, :]
    ).astype(jnp.float32)
    shares = lax.psum_scatter(entry_grads, "tp", scatter_dimension=1, tiled=True)
    summed = jnp.einsum("ep,ekc->pkc", spread, shares, precision=lax.Precision.HIGHEST)
    key_share = summed.shape[1]
    returned = lax.all_to_all(
        summed[:slot_count].reshape(kv_count, CAP, key_share, 2 * DH).astype(jnp.bfloat16),
        "kv",
        split_axis=0,
        concat_axis=0,
        tiled=True,
    ).astype(jnp.float32)
    keyval_grad = (
        jnp.einsum(
            "rsb,rskc->bkc",
            owner_slots.astype(jnp.float32),
            returned,
            precision=lax.Precision.HIGHEST,
        )
        + summed[slot_count:]
    )
    weight_grad = lax.psum_scatter(
        weight_term(inputs, query_grad), "kv", scatter_dimension=0, tiled=True
    )
    return (query_grad, keyval_grad, weight_grad)


def bit_orders(kv_count, chunk_count):
    bits = kv_count.bit_length() - 1
    orders = []
    for c in range(chunk_count):
        turn = c % 3
        first = [0, 1, 2]
        orders.append(first[turn:] + first[:turn] + list(range(3, bits)))
    return orders


def flip(index, place):
    bit = (index // (1 << place)) % 2
    return index + (1 - 2 * bit) * (1 << place)


def fused_kernel(
    kv_count,
    orders,
    sel_hbm,
    own_hbm,
    log_hbm,
    q_hbm,
    g_hbm,
    in_hbm,
    qg_ref,
    wg_ref,
    kvg_ref,
    sel_scr,
    first_scr,
    table_scr,
    first_ref,
    table_ref,
    out_scr,
    log_ref,
    own_scr,
    q_scr,
    g_scr,
    in_scr,
    pool_scr,
    kk_scr,
    vv_scr,
    kt_scr,
    qm_scr,
    gm_scr,
    ds_scr,
    pb_scr,
    dkv_scr,
    qgt_scr,
    total,
    half_scr,
    tp_scr,
    slot_scr,
    ret_scr,
    *rest,
):
    bits = len(orders[0])
    chunk_count = len(orders)
    send_scr = rest[:bits]
    recv_scr = rest[bits : 2 * bits]
    load_sem, get_send, get_recv, tp_send, tp_recv, ret_send, ret_recv, w_send, w_recv = rest[2 * bits :]
    me = lax.axis_index("kv")
    core = lax.axis_index("tp")
    other = 1 - core
    rows, width = wg_ref.shape
    pair_count = width // (2 * DH * GROUP)
    per_dev = q_scr.shape[0] // QB
    slot_count = kv_count * CAP
    entry_count = per_dev * NSEL
    diagonal = QB // KB
    half = KB // 2
    score_scale = DH ** (-0.5)

    def peer(step):
        return lax.rem(me + step, kv_count)

    own_blocks = own_hbm.shape[0]
    loads = [
        pltpu.make_async_copy(src, dst, load_sem.at[i])
        for i, (src, dst) in enumerate(
            (
                (sel_hbm, sel_scr),
                (own_hbm, own_scr),
                (log_hbm, log_ref),
                (q_hbm, q_scr),
                (g_hbm, g_scr),
                (in_hbm, in_scr),
                (first_scr, first_ref),
                (table_scr, table_ref),
            )
        )
    ]
    for load in loads[:6]:
        load.start()
    pool_scr[...] = jnp.zeros(pool_scr.shape, jnp.bfloat16)
    ret_scr[...] = jnp.zeros(ret_scr.shape, jnp.bfloat16)

    barrier = pltpu.get_barrier_semaphore()
    for step in range(1, kv_count):
        pl.semaphore_signal(barrier, inc=1, device_id=(peer(step), core), device_id_type=MESH)
    pl.semaphore_signal(barrier, inc=1, device_id=(me, other), device_id_type=MESH)

    loads[0].wait()
    chosen = padded(sel_scr[...])
    first_scr[...] = first_table(chosen, me * own_blocks, own_blocks, per_dev)
    loads[6].start()
    table_scr[...] = entry_table(chosen, me, kv_count, own_blocks, per_dev)
    loads[7].start()
    dkv_scr[entry_count] = jnp.zeros((KB, 2 * DH), jnp.float32)
    loads[1].wait()
    loads[6].wait()
    for r in range(kv_count):
        for s in range(CAP):
            out_scr[r, s] = own_scr[first_ref[s, r * per_dev]]
    pl.semaphore_wait(barrier, kv_count)

    def get_copy(target, source):
        return pltpu.make_async_remote_copy(
            src_ref=out_scr.at[target],
            dst_ref=pool_scr.at[pl.ds(source * CAP, CAP)],
            send_sem=get_send.at[target],
            recv_sem=get_recv.at[source],
            device_id=(target, core),
            device_id_type=MESH,
        )

    def later(do):
        for step in range(kv_count - 1, 0, -1):
            @pl.when(me + step < kv_count)
            def _():
                do(me + step)

    def earlier(do):
        for step in range(1, kv_count):
            @pl.when(me >= step)
            def _():
                do(me - step)

    later(lambda r: get_copy(r, me).start())
    for load in loads[2:5]:
        load.wait()
    low_half = lax.broadcasted_iota(jnp.int32, (QB, 2 * DH), 1) < DH

    def prepare(p, carry):
        tok = pl.ds(pl.multiple_of(p * QB, QB), QB)
        for pair in range(pair_count):
            cols = slice(pair * 2 * DH, (pair + 1) * 2 * DH)
            for src, dst, scale in ((q_scr, qm_scr, score_scale), (g_scr, gm_scr, 1.0)):
                both = src[tok, cols] * jnp.asarray(scale, jnp.bfloat16)
                zero = jnp.zeros_like(both)
                at = pair * 2 * QB
                dst[p, at : at + QB, :] = jnp.where(low_half, both, zero)
                dst[p, at + QB : at + 2 * QB, :] = jnp.where(low_half, zero, both)
        return carry

    lax.fori_loop(0, per_dev, prepare, 0)
    loads[7].wait()
    earlier(lambda r: get_copy(me, r).wait_recv())
    low_key = lax.broadcasted_iota(jnp.int32, (KB, 2 * DH), 1) < DH

    def gather(p, carry):
        for e in range(NSEL):
            rows = slice(e * KB, (e + 1) * KB)
            both = own_scr[p * diagonal + e] if e < diagonal else pool_scr[table_ref[e, p]]
            turned = jnp.concatenate([both[:, DH:], both[:, :DH]], axis=1)
            kk_scr[p, rows, :] = jnp.where(low_key, both, turned)
            vv_scr[p, rows, :] = jnp.where(low_key, turned, both)
        kt_scr[p] = kk_scr[p][:, :DH].T * jnp.asarray(score_scale, jnp.bfloat16)
        return carry

    lax.fori_loop(0, per_dev, gather, 0)

    key_row = lax.broadcasted_iota(jnp.int32, (QB, 2 * QB), 0)
    query_col = lax.broadcasted_iota(jnp.int32, (QB, 2 * QB), 1) % QB
    causal = key_row <= query_col
    nt = (((1,), (1,)), ((), ()))

    def attend(pair):
        at = pair * 2 * DH
        heads = slice(pair * 2 * QB, (pair + 1) * 2 * QB)
        rows = NSEL * KB // 1

        def multiply(p, h):
            keys = slice(h * rows, (h + 1) * rows)
            scores = lax.dot_general(
                kk_scr[p, keys, :], qm_scr[p, heads, :], nt, preferred_element_type=jnp.float32
            )
            dprob = lax.dot_general(
                vv_scr[p, keys, :], gm_scr[p, heads, :], nt, preferred_element_type=jnp.float32
            )
            return scores, dprob

        def weigh(p, h, scores, dprob):
            tok = slice(p * QB, (p + 1) * QB)
            log2 = jnp.concatenate(
                [log_ref[2 * pair : 2 * pair + 1, tok], log_ref[2 * pair + 1 : 2 * pair + 2, tok]], axis=1
            )
            log2 = log2 * LOG2E
            parts = []
            for i in range(rows // KB):
                e = h * (rows // KB) + i
                penalty = jnp.where(table_ref[NSEL + e, p] >= 0, jnp.float32(0.0), jnp.float32(DEAD))
                part = scores[i * KB : (i + 1) * KB] * LOG2E - (log2 + penalty)
                if e < diagonal:
                    part = jnp.where(causal[e * KB : (e + 1) * KB], part, -DEAD)
                parts.append(part)
            prob = jnp.exp2(jnp.concatenate(parts, axis=0))
            prob_b = prob.astype(jnp.bfloat16)
            pb_scr[p, h * rows : (h + 1) * rows, heads] = prob_b
            seen = prob_b.astype(jnp.float32)
            delta = jnp.sum(seen * dprob, axis=0, keepdims=True)

            return prob, delta

        def finish_block(p, probs, dprobs, delta):
            tok = slice(p * QB, (p + 1) * QB)
            dq = None
            for h in range(1):
                keys = slice(h * rows, (h + 1) * rows)
                prob, dprob = probs[h], dprobs[h]
                dscore_b = (prob * (dprob - delta)).astype(jnp.bfloat16)
                ds_scr[p, keys, heads] = dscore_b
            dq = jnp.dot(kt_scr[p], ds_scr[p, :, heads], preferred_element_type=jnp.float32)
            dq = jnp.concatenate([dq[:, :QB], dq[:, QB:]], axis=0)
            qgt_scr[at : at + 2 * DH, tok] = dq.astype(jnp.bfloat16)
            qg_ref[tok, at : at + 2 * DH] = dq.T.astype(jnp.bfloat16)

        ready = multiply(0, 0)
        for p in range(per_dev):
            now = ready
            ready = multiply(p + 1, 0) if p + 1 < per_dev else None
            prob, delta = weigh(p, 0, *now)
            finish_block(p, [prob], [now[1]], delta)

    low_row = lax.broadcasted_iota(jnp.int32, (NSEL * KB, 2 * DH), 1) < DH

    def key_value(p, carry):
        dk = jnp.dot(ds_scr[p], qm_scr[p], preferred_element_type=jnp.float32)
        dv = jnp.dot(pb_scr[p], gm_scr[p], preferred_element_type=jnp.float32)
        near = jnp.where(low_row, dk, dv)
        far = jnp.where(low_row, dv, dk)
        dkv = near + pltpu.roll(far, DH, 1)
        dkv_scr[pl.ds(p * NSEL, NSEL)] = dkv.reshape(NSEL, KB, 2 * DH)
        return carry

    def product(pair):
        cols = slice(pair * GROUP * 2 * DH, (pair + 1) * GROUP * 2 * DH)

        def piece(j, carry):
            at = pl.multiple_of(j * 2 * rows, 2 * rows)
            part = jnp.dot(
                qgt_scr[cols, :], in_scr[:, pl.ds(at, 2 * rows)], preferred_element_type=jnp.float32
            )
            total[2 * j, cols, :] = part[:, :rows]
            total[2 * j + 1, cols, :] = part[:, rows:]
            return carry

        lax.fori_loop(0, kv_count // 2, piece, 0, unroll=PIECES)

    def owner_of(c, slot):
        owner = me
        for k in range(bits):
            if (slot >> (bits - 1 - k)) & 1:
                owner = flip(owner, orders[c][k])
        return owner

    def current(c, slot, k):
        at = owner_of(c, slot)
        value = total[at, c * DH : (c + 1) * DH, :]
        if k > 0:
            value = value + recv_scr[k - 1][c, slot].astype(jnp.float32)
            total[at, c * DH : (c + 1) * DH, :] = value
        return value

    def weight_copy(c, k):
        return pltpu.make_async_remote_copy(
            src_ref=send_scr[k].at[c],
            dst_ref=recv_scr[k].at[c],
            send_sem=w_send.at[c, k],
            recv_sem=w_recv.at[c, k],
            device_id=(flip(me, orders[c][k]), core),
            device_id_type=MESH,
        )

    def weight_stage(pair, k):
        left = kv_count >> (k + 1)
        for c in range(2 * GROUP * pair, 2 * GROUP * (pair + 1)):
            if k > 0:
                weight_copy(c, k - 1).wait_recv()
            if k == bits:
                value = total[me, c * DH : (c + 1) * DH, :] + recv_scr[k - 1][c, 0].astype(jnp.float32)
                wg_ref[:, c * DH : (c + 1) * DH] = value.T
                continue
            for slot in range(left, 2 * left):
                send_scr[k][c, slot - left] = current(c, slot, k).astype(jnp.bfloat16)
            weight_copy(c, k).start()
            if k > 0:
                for slot in range(left):
                    current(c, slot, k)

    def advance(turn):
        for k in range(bits + 1):
            if 0 <= turn - k < pair_count:
                weight_stage(turn - k, k)

    tp_copy = pltpu.make_async_remote_copy(
        src_ref=half_scr.at[other],
        dst_ref=tp_scr,
        send_sem=tp_send,
        recv_sem=tp_recv,
        device_id=(me, other),
        device_id_type=MESH,
    )

    def ret_copy(target, source):
        return pltpu.make_async_remote_copy(
            src_ref=slot_scr.at[target],
            dst_ref=ret_scr.at[source],
            send_sem=ret_send.at[target],
            recv_sem=ret_recv.at[source],
            device_id=(target, core),
            device_id_type=MESH,
        )

    def collect(s, carry):
        value = dkv_scr[table_ref[2 * NSEL + s, 0]]
        for p in range(1, per_dev):
            value = value + dkv_scr[table_ref[2 * NSEL + s, p]]
        half_scr[0, s] = value[:half]
        half_scr[1, s] = value[half:]
        return carry

    for pair in range(pair_count):
        attend(pair)
        if pair == 0:
            loads[5].wait()
        product(pair)
        advance(pair)
    lax.fori_loop(0, per_dev, key_value, 0, unroll=KEYS)
    lax.fori_loop(0, slot_count, collect, 0)
    for p in range(per_dev):
        at = slot_count + p * diagonal
        half_scr[0, at : at + diagonal] = dkv_scr[p * NSEL : p * NSEL + diagonal, :half, :]
        half_scr[1, at : at + diagonal] = dkv_scr[p * NSEL : p * NSEL + diagonal, half:, :]
    tp_copy.start()
    advance(pair_count)

    tp_copy.wait_recv()
    mine = half_scr.at[core]
    slot_scr[...] = (
        (mine[:slot_count] + tp_scr[:slot_count])
        .astype(jnp.bfloat16)
        .reshape(kv_count, CAP, half, 2 * DH)
    )
    earlier(lambda r: ret_copy(r, me).start())
    own_sum = (mine[slot_count:] + tp_scr[slot_count:]).reshape(own_blocks * half, 2 * DH)

    for turn in range(pair_count + 1, pair_count + bits):
        advance(turn)
    later(lambda r: ret_copy(me, r).wait_recv())
    column = lax.broadcasted_iota(jnp.int32, (1, slot_count * half), 1)
    block = jnp.zeros(column.shape, jnp.int32)
    for r in range(kv_count):
        for s in range(CAP):
            block = jnp.where(column // half == r * CAP + s, first_ref[s, r * per_dev], block)
    wanted = block * half + column % half
    row = lax.broadcasted_iota(jnp.int32, (own_blocks * half, slot_count * half), 0)
    spread = jnp.where(row == wanted, 1.0, 0.0).astype(jnp.bfloat16)
    back = ret_scr[...].reshape(slot_count * half, 2 * DH)
    kvg = own_sum + jnp.dot(spread, back, preferred_element_type=jnp.float32)
    kvg_ref[...] = kvg.reshape(own_blocks, half, 2 * DH)
    later(lambda r: get_copy(r, me).wait_send())
    earlier(lambda r: ret_copy(r, me).wait_send())
    tp_copy.wait_send()
    for c in range(chunk_count):
        for k in range(bits):
            weight_copy(c, k).wait_send()


def padded(chosen):
    fill = jnp.full((NSEL, 128 - chosen.shape[1]), -1, jnp.int32)
    return jnp.concatenate([chosen, fill], axis=1)


def first_table(chosen, base, own_blocks, per_dev):
    inside = (chosen >= base) & (chosen < base + own_blocks)
    low = jnp.min(jnp.where(inside, chosen - base, own_blocks), axis=0, keepdims=True)
    high = jnp.max(jnp.where(inside, chosen - base, -1), axis=0, keepdims=True)
    cover = 1
    while cover < per_dev:
        shift = 128 - min(cover, per_dev - cover)
        low = jnp.minimum(low, pltpu.roll(low, shift, 1))
        high = jnp.maximum(high, pltpu.roll(high, shift, 1))
        cover = min(2 * cover, per_dev)
    low = jnp.where(low == own_blocks, 0, low)
    high = jnp.maximum(high, 0)
    row = lax.broadcasted_iota(jnp.int32, (8, 128), 0)
    return jnp.where(row == 0, low, high)


def entry_table(chosen, me, kv_count, own_blocks, per_dev):
    slot_count = kv_count * CAP
    spare = per_dev * NSEL
    lane = lax.broadcasted_iota(jnp.int32, (NSEL, 128), 1)
    entry = lax.broadcasted_iota(jnp.int32, (NSEL, 128), 0) + lane * NSEL
    blocks = pltpu.roll(chosen, lax.rem(128 - me * per_dev + 128, 128), 1)
    blocks = jnp.where(lane < per_dev, blocks, -1)
    top = kv_count * own_blocks
    lows = []
    for o in range(kv_count):
        inside = (blocks >= o * own_blocks) & (blocks < (o + 1) * own_blocks)
        lows.append(jnp.min(jnp.where(inside, blocks, top), axis=0, keepdims=True))
    low = jnp.min(jnp.concatenate(lows, axis=0), axis=1, keepdims=True)
    slot = jnp.full((NSEL, 128), slot_count, jnp.int32)
    for o in range(kv_count):
        inside = (blocks >= o * own_blocks) & (blocks < (o + 1) * own_blocks)
        at = o * CAP + jnp.where(blocks > low[o : o + 1], 1, 0)
        slot = jnp.where(inside, at, slot)
    mine = (blocks >= me * own_blocks) & (blocks < (me + 1) * own_blocks)
    slot = jnp.where(mine, slot_count, slot)
    places = []
    for s in range(slot_count):
        found = jnp.max(jnp.where(slot == s, entry, -1), axis=0, keepdims=True)
        places.append(jnp.where(found < 0, spare, found))
    return jnp.concatenate([jnp.minimum(slot, slot_count - 1), blocks] + places, axis=0)


def finish_kernel(qg_ref, wg_ref, kvg_ref, qg_out, wg_out, kvg_out, sem):
    pairs = ((qg_ref, qg_out), (wg_ref, wg_out), (kvg_ref, kvg_out))
    copies = [pltpu.make_async_copy(src, dst, sem.at[i]) for i, (src, dst) in enumerate(pairs)]
    for copy in copies:
        copy.start()
    for copy in copies:
        copy.wait()


def finish(*results):
    hbm = pl.BlockSpec(memory_space=pl.ANY)
    return pl.pallas_call(
        finish_kernel,
        out_shape=[jax.ShapeDtypeStruct(r.shape, r.dtype) for r in results],
        in_specs=[hbm] * 3,
        out_specs=[hbm] * 3,
        scratch_shapes=[pltpu.SemaphoreType.DMA((3,))],
        compiler_params=pltpu.CompilerParams(vmem_limit_bytes=1024 * 1024),
        name="finish",
    )(*results)


def fused(kv_count, chosen, own_kv, log_sums, queries, out_grad, inputs):
    operands = (chosen, own_kv, log_sums, queries, out_grad, inputs)
    tok_count, width = queries.shape
    per_dev = tok_count // QB
    rows = inputs.shape[1] // kv_count
    chunk_count = width // DH
    orders = bit_orders(kv_count, chunk_count)
    bits = len(orders[0])
    slot_count = kv_count * CAP
    pool_count = slot_count + own_kv.shape[0]
    half = KB // 2
    parts = [
        pltpu.VMEM((chunk_count, kv_count >> (k + 1), DH, rows), jnp.bfloat16) for k in range(bits)
    ]
    vmem = pl.BlockSpec(memory_space=pltpu.VMEM)
    hbm = pl.BlockSpec(memory_space=pl.ANY)
    dma = pltpu.SemaphoreType.DMA
    table_rows = 2 * NSEL + slot_count
    return pl.pallas_call(
        functools.partial(fused_kernel, kv_count, orders),
        out_shape=[
            pltpu.VMEM((tok_count, width), jnp.bfloat16),
            pltpu.VMEM((rows, width), jnp.float32),
            pltpu.VMEM((own_kv.shape[0], half, 2 * DH), jnp.float32),
        ],
        in_specs=[hbm] * 6,
        out_specs=[vmem] * 3,
        scratch_shapes=[
            pltpu.VMEM(chosen.shape, jnp.int32),
            pltpu.VMEM((8, 128), jnp.int32),
            pltpu.VMEM((table_rows, 128), jnp.int32),
            pltpu.SMEM((8, 128), jnp.int32),
            pltpu.SMEM((table_rows, 128), jnp.int32),
            pltpu.VMEM((kv_count, CAP, KB, 2 * DH), jnp.bfloat16),
            pltpu.VMEM(log_sums.shape, jnp.float32),
            pltpu.VMEM(own_kv.shape, jnp.bfloat16),
            pltpu.VMEM((tok_count, width), jnp.bfloat16),
            pltpu.VMEM((tok_count, width), jnp.bfloat16),
            pltpu.VMEM(inputs.shape, jnp.bfloat16),
            pltpu.VMEM((slot_count, KB, 2 * DH), jnp.bfloat16),
            pltpu.VMEM((per_dev, NSEL * KB, 2 * DH), jnp.bfloat16),
            pltpu.VMEM((per_dev, NSEL * KB, 2 * DH), jnp.bfloat16),
            pltpu.VMEM((per_dev, DH, NSEL * KB), jnp.bfloat16),
            pltpu.VMEM((per_dev, QB * width // DH, 2 * DH), jnp.bfloat16),
            pltpu.VMEM((per_dev, QB * width // DH, 2 * DH), jnp.bfloat16),
            pltpu.VMEM((per_dev, NSEL * KB, QB * width // DH), jnp.bfloat16),
            pltpu.VMEM((per_dev, NSEL * KB, QB * width // DH), jnp.bfloat16),
            pltpu.VMEM((per_dev * NSEL + 1, KB, 2 * DH), jnp.float32),
            pltpu.VMEM((width, tok_count), jnp.bfloat16),
            pltpu.VMEM((kv_count, width, rows), jnp.float32),
            pltpu.VMEM((2, pool_count, half, 2 * DH), jnp.float32),
            pltpu.VMEM((pool_count, half, 2 * DH), jnp.float32),
            pltpu.VMEM((kv_count, CAP, half, 2 * DH), jnp.bfloat16),
            pltpu.VMEM((kv_count, CAP, half, 2 * DH), jnp.bfloat16),
        ]
        + parts
        + parts
        + [
            dma((8,)),
            dma((kv_count,)),
            dma((kv_count,)),
            dma,
            dma,
            dma((kv_count,)),
            dma((kv_count,)),
            dma((chunk_count, bits)),
            dma((chunk_count, bits)),
        ],
        compiler_params=pltpu.CompilerParams(
            collective_id=0, has_side_effects=True, vmem_limit_bytes=VMEM_LIMIT
        ),
        name="fused",
    )(*(pltpu.with_memory_space_constraint(x, pltpu.HBM) for x in operands))


def fused_body(queries, keyvals, log_sums, out_grad, inputs, selection):
    kv_count = lax.axis_size("kv")
    own_blocks = queries.shape[0] // KB
    own_kv = keyvals.reshape(own_blocks, KB, 2 * DH)
    results = fused(kv_count, selection.T, own_kv, log_sums, queries, out_grad, inputs)
    query_grad, weight_grad, keyval_grad = finish(*results)
    return (query_grad, keyval_grad, weight_grad)


def fits(kv_count, tp_count, tok_count, rows, width):
    power = kv_count & (kv_count - 1) == 0 and kv_count >= 8
    lanes = power and kv_count <= NSEL and kv_count * (tok_count // QB) <= 128
    return tp_count == 2 and lanes and rows % 128 == 0 and width % (2 * DH * GROUP) == 0


def step(queries, keyvals, log_sums, out_grad, inputs, selection):
    kv_count, tp_count = lax.axis_size("kv"), lax.axis_size("tp")
    chosen = fits(kv_count, tp_count, queries.shape[0], inputs.shape[1] // kv_count, queries.shape[1])
    return (fused_body if chosen else body)(
        queries, keyvals, log_sums, out_grad, inputs, selection
    )


def solution(mesh):
    return jax.shard_map(
        step,
        mesh=mesh,
        in_specs=(P("kv", "tp"), P("kv", None), P("tp", "kv"), P("kv", "tp"), P("kv", None), P()),
        out_specs=(P("kv", "tp"), P("kv", "tp", None), P("kv", "tp")),
        check_vma=False,
    )
```

```python
import functools

import jax
import jax.numpy as jnp
from jax import lax
from jax.experimental import pallas as pl
from jax.experimental.pallas import tpu as pltpu
from jax.sharding import PartitionSpec as P

DH = 64
QB = 128
KB = 32
NSEL = 16
CAP = 2
LOG2E = 1.4426950408889634
DEAD = 1e30
GROUP = 1
UNROLL = True
PIECES = 8
HOP_US = (5.5, 4.0, 3.5, 4.0)
LAST_US = (5.5, 4.0, 3.5, 4.0)
PAIR_US = 2.95
KEY_US = 0.78
TP_US = 7.4
KEYS = 7
VMEM_LIMIT = 48 * 1024 * 1024
MESH = pl.DeviceIdType.MESH


def slot_table(wanted):
    slot_rank = jnp.cumsum(wanted.astype(jnp.int32), axis=1) - 1
    return wanted[:, None, :] & (
        slot_rank[:, None, :] == jnp.arange(CAP, dtype=jnp.int32)[None, :, None]
    )


def weight_term(inputs, query_grad):
    return lax.dot_general(
        inputs, query_grad, (((0,), (0,)), ((), ())), preferred_element_type=jnp.float32
    )


def body(queries, keyvals, log_sums, out_grad, inputs, selection):
    kv_count = lax.axis_size("kv")
    own_index = lax.axis_index("kv")
    tok_count, width = queries.shape
    head_count = width // DH
    per_dev = tok_count // QB
    own_blocks = tok_count // KB
    slot_count = kv_count * CAP
    score_scale = DH ** (-0.5)
    own_kv = keyvals.reshape(own_blocks, KB, 2 * DH)
    lists = selection.reshape(kv_count, per_dev * NSEL)
    device_ids = jnp.arange(kv_count, dtype=jnp.int32)
    mine = own_index * own_blocks + jnp.arange(own_blocks, dtype=jnp.int32)
    wanted = jnp.any(lists[:, :, None] == mine[None, None, :], axis=1) & (
        device_ids[:, None] != own_index
    )
    owner_slots = slot_table(wanted)
    outgoing = jnp.einsum(
        "rsb,bkc->rskc",
        owner_slots.astype(jnp.bfloat16),
        own_kv,
        preferred_element_type=jnp.float32,
    ).astype(jnp.bfloat16)
    fetched = lax.all_to_all(outgoing, "kv", split_axis=0, concat_axis=0, tiled=True)
    block_list = lax.dynamic_index_in_dim(lists, own_index, 0, keepdims=False)
    every_block = jnp.arange(kv_count * own_blocks, dtype=jnp.int32)
    hits = block_list[:, None] == every_block[None, :]
    needed = jnp.any(hits, axis=0).reshape(kv_count, own_blocks) & (
        device_ids[:, None] != own_index
    )
    slot_rank = jnp.cumsum(needed.astype(jnp.int32), axis=1) - 1
    entry_rank = jnp.sum(jnp.where(hits, slot_rank.reshape(-1)[None, :], 0), axis=1)
    safe_list = jnp.maximum(block_list, 0)
    owner_index = safe_list // own_blocks
    local_block = safe_list % own_blocks
    pool_index = jnp.where(
        owner_index == own_index, slot_count + local_block, owner_index * CAP + entry_rank
    )
    pool_index = jnp.where(block_list < 0, 0, pool_index)
    block_pool = jnp.concatenate([fetched.reshape(slot_count, KB, 2 * DH), own_kv], axis=0)
    gathered = jnp.take(block_pool, pool_index, axis=0).reshape(per_dev, NSEL * KB, 2 * DH)
    key_rows = gathered[:, :, :DH]
    value_rows = gathered[:, :, DH:]
    query_rows = queries.reshape(per_dev, QB, head_count, DH)
    grad_rows = out_grad.reshape(per_dev, QB, head_count, DH)
    log_rows = log_sums.reshape(head_count, per_dev, QB).transpose(1, 0, 2)
    key_pos = (
        safe_list.reshape(per_dev, NSEL, 1) * KB + jnp.arange(KB, dtype=jnp.int32)[None, None, :]
    ).reshape(per_dev, NSEL * KB)
    key_live = jnp.repeat((block_list >= 0).reshape(per_dev, NSEL), KB, axis=1)
    query_pos = own_index * tok_count + jnp.arange(tok_count, dtype=jnp.int32).reshape(per_dev, QB)
    live_mask = key_live[:, None, :] & (key_pos[:, None, :] <= query_pos[:, :, None])
    scores = (
        jnp.einsum("pthd,pkd->phtk", query_rows, key_rows, preferred_element_type=jnp.float32)
        * score_scale
    )
    prob_f32 = jnp.where(live_mask[:, None], jnp.exp(scores - log_rows[..., None]), 0.0)
    prob_b = prob_f32.astype(jnp.bfloat16)
    recomputed = jnp.einsum(
        "phtk,pkd->pthd", prob_b, value_rows, preferred_element_type=jnp.float32
    )
    row_delta = jnp.sum(grad_rows.astype(jnp.float32) * recomputed, axis=-1)
    dprob = jnp.einsum("pthd,pkd->phtk", grad_rows, value_rows, preferred_element_type=jnp.float32)
    dscore = prob_f32 * (dprob - row_delta.transpose(0, 2, 1)[..., None])
    dscore_b = dscore.astype(jnp.bfloat16)
    query_grad = (
        (
            jnp.einsum("phtk,pkd->pthd", dscore_b, key_rows, preferred_element_type=jnp.float32)
            * score_scale
        )
        .astype(jnp.bfloat16)
        .reshape(tok_count, width)
    )
    key_grad = (
        jnp.einsum("phtk,pthd->pkd", dscore_b, query_rows, preferred_element_type=jnp.float32)
        * score_scale
    )
    value_grad = jnp.einsum("phtk,pthd->pkd", prob_b, grad_rows, preferred_element_type=jnp.float32)
    entry_grads = jnp.concatenate([key_grad, value_grad], axis=-1).reshape(
        per_dev * NSEL, KB, 2 * DH
    )
    spread = (
        pool_index[:, None] == jnp.arange(slot_count + own_blocks, dtype=jnp.int32)[None, :]
    ).astype(jnp.float32)
    shares = lax.psum_scatter(entry_grads, "tp", scatter_dimension=1, tiled=True)
    summed = jnp.einsum("ep,ekc->pkc", spread, shares, precision=lax.Precision.HIGHEST)
    key_share = summed.shape[1]
    returned = lax.all_to_all(
        summed[:slot_count].reshape(kv_count, CAP, key_share, 2 * DH).astype(jnp.bfloat16),
        "kv",
        split_axis=0,
        concat_axis=0,
        tiled=True,
    ).astype(jnp.float32)
    keyval_grad = (
        jnp.einsum(
            "rsb,rskc->bkc",
            owner_slots.astype(jnp.float32),
            returned,
            precision=lax.Precision.HIGHEST,
        )
        + summed[slot_count:]
    )
    weight_grad = lax.psum_scatter(
        weight_term(inputs, query_grad), "kv", scatter_dimension=0, tiled=True
    )
    return (query_grad, keyval_grad, weight_grad)


def bit_orders(kv_count, chunk_count):
    bits = kv_count.bit_length() - 1
    orders = []
    for c in range(chunk_count):
        turn = c % 3
        first = [0, 1, 2]
        orders.append(first[turn:] + first[:turn] + list(range(3, bits)))
    return orders


def plan(pair_count, per_dev, bits):
    points = []
    for pair in range(pair_count):
        points += [("mid", pair, PAIR_US * (pair + 0.5)), ("end", pair, PAIR_US * (pair + 1))]
    last = PAIR_US * pair_count
    points += [("key", p, last + KEY_US * (p + 1)) for p in range(per_dev)]
    chosen, sends, finals = {}, [], []
    for pair in range(pair_count):
        hops = LAST_US if pair == pair_count - 1 else HOP_US
        lags = hops[: bits - 1] + hops[-1:]
        chosen.setdefault(("end", pair), []).append((pair, 0))
        ready = PAIR_US * (pair + 1)
        for k, lag in enumerate(lags):
            ready += lag
            fitting = [point for point in points if point[2] >= ready]
            if fitting and k + 1 < len(lags):
                chosen.setdefault(fitting[0][:2], []).append((pair, k + 1))
                ready = fitting[0][2]
            elif k + 1 < len(lags):
                sends.append((ready - last, pair, k + 1))
            else:
                finals.append((ready - last, pair, k + 1))
    return chosen, sorted(sends), finals


def flip(index, place):
    bit = (index // (1 << place)) % 2
    return index + (1 - 2 * bit) * (1 << place)


def fused_kernel(
    kv_count,
    orders,
    sel_hbm,
    own_hbm,
    log_hbm,
    q_hbm,
    g_hbm,
    in_hbm,
    qg_ref,
    wg_ref,
    kvg_ref,
    sel_scr,
    first_scr,
    table_scr,
    first_ref,
    table_ref,
    out_scr,
    log_ref,
    own_scr,
    q_scr,
    g_scr,
    in_scr,
    pool_scr,
    kk_scr,
    vv_scr,
    kt_scr,
    qm_scr,
    gm_scr,
    ds_scr,
    pb_scr,
    dkv_scr,
    qgt_scr,
    total,
    half_scr,
    tp_scr,
    slot_scr,
    ret_scr,
    *rest,
):
    bits = len(orders[0])
    chunk_count = len(orders)
    send_scr = rest[:bits]
    recv_scr = rest[bits : 2 * bits]
    load_sem, get_send, get_recv, tp_send, tp_recv, ret_send, ret_recv, w_send, w_recv = rest[2 * bits :]
    me = lax.axis_index("kv")
    core = lax.axis_index("tp")
    other = 1 - core
    rows, width = wg_ref.shape
    pair_count = width // (2 * DH * GROUP)
    per_dev = q_scr.shape[0] // QB
    slot_count = kv_count * CAP
    entry_count = per_dev * NSEL
    diagonal = QB // KB
    half = KB // 2
    score_scale = DH ** (-0.5)

    def peer(step):
        return lax.rem(me + step, kv_count)

    own_blocks = own_hbm.shape[0]
    loads = [
        pltpu.make_async_copy(src, dst, load_sem.at[i])
        for i, (src, dst) in enumerate(
            (
                (sel_hbm, sel_scr),
                (own_hbm, own_scr),
                (log_hbm, log_ref),
                (q_hbm, q_scr),
                (g_hbm, g_scr),
                (in_hbm, in_scr),
                (first_scr, first_ref),
                (table_scr, table_ref),
            )
        )
    ]
    for load in loads[:6]:
        load.start()
    pool_scr[me] = jnp.zeros(pool_scr.shape[1:], jnp.bfloat16)
    ret_scr[me] = jnp.zeros(ret_scr.shape[1:], jnp.bfloat16)

    barrier = pltpu.get_barrier_semaphore()
    for step in range(1, kv_count):
        pl.semaphore_signal(barrier, inc=1, device_id=(peer(step), core), device_id_type=MESH)
    pl.semaphore_signal(barrier, inc=1, device_id=(me, other), device_id_type=MESH)

    loads[0].wait()
    chosen = padded(sel_scr[...])
    first_scr[...] = first_table(chosen, me * own_blocks, own_blocks, per_dev)
    loads[6].start()
    table_scr[...] = entry_table(chosen, me, kv_count, own_blocks, per_dev)
    loads[7].start()
    dkv_scr[entry_count] = jnp.zeros((KB, 2 * DH), jnp.float32)
    loads[1].wait()
    loads[6].wait()
    for r in range(kv_count):
        for s in range(CAP):
            out_scr[r, s] = own_scr[first_ref[s, r * per_dev]]
    pl.semaphore_wait(barrier, kv_count)

    def exchange(send, receive, sems):
        def copy(src_ref, dst_ref, target):
            return pltpu.make_async_remote_copy(
                src_ref=src_ref,
                dst_ref=dst_ref,
                send_sem=sems[0],
                recv_sem=sems[1],
                device_id=(target, core),
                device_id_type=MESH,
            )

        def start():
            for step in range(kv_count - 1, 0, -1):
                copy(send.at[peer(step)], receive.at[me], peer(step)).start()

        every = copy(send.at[: kv_count - 1], receive.at[: kv_count - 1], peer(1))
        return start, every

    get_start, get_every = exchange(out_scr, pool_scr, (get_send, get_recv))
    get_start()
    for load in loads[2:5]:
        load.wait()
    low_half = lax.broadcasted_iota(jnp.int32, (QB, 2 * DH), 1) < DH

    def prepare(p, carry):
        tok = pl.ds(pl.multiple_of(p * QB, QB), QB)
        for pair in range(pair_count):
            cols = slice(pair * 2 * DH, (pair + 1) * 2 * DH)
            for src, dst, scale in ((q_scr, qm_scr, score_scale), (g_scr, gm_scr, 1.0)):
                both = src[tok, cols] * jnp.asarray(scale, jnp.bfloat16)
                zero = jnp.zeros_like(both)
                at = pair * 2 * QB
                dst[p, at : at + QB, :] = jnp.where(low_half, both, zero)
                dst[p, at + QB : at + 2 * QB, :] = jnp.where(low_half, zero, both)
        return carry

    lax.fori_loop(0, per_dev, prepare, 0)
    low_key = lax.broadcasted_iota(jnp.int32, (KB, 2 * DH), 1) < DH
    key_scale = jnp.asarray(score_scale, jnp.bfloat16)

    def spread_block(p, e, both):
        rows = slice(e * KB, (e + 1) * KB)
        turned = jnp.concatenate([both[:, DH:], both[:, :DH]], axis=1)
        kk_scr[p, rows, :] = jnp.where(low_key, both, turned)
        vv_scr[p, rows, :] = jnp.where(low_key, turned, both)

    for p in range(per_dev):
        for e in range(diagonal):
            spread_block(p, e, own_scr[p * diagonal + e])
        kt_scr[p, :, :QB] = kk_scr[p, :QB, :DH].T * key_scale
    loads[7].wait()
    get_every.wait_recv()
    for p in range(per_dev):
        for e in range(diagonal, NSEL):
            spread_block(p, e, pool_scr[table_ref[e, p], table_ref[2 * NSEL + slot_count + e, p]])
        kt_scr[p, :, QB:] = kk_scr[p, QB:, :DH].T * key_scale

    key_row = lax.broadcasted_iota(jnp.int32, (QB, 2 * QB), 0)
    query_col = lax.broadcasted_iota(jnp.int32, (QB, 2 * QB), 1) % QB
    causal = key_row <= query_col
    nt = (((1,), (1,)), ((), ()))

    def attend(pair):
        at = pair * 2 * DH
        heads = slice(pair * 2 * QB, (pair + 1) * 2 * QB)
        rows = NSEL * KB // 1

        def multiply(p, h):
            keys = slice(h * rows, (h + 1) * rows)
            scores = lax.dot_general(
                kk_scr[p, keys, :], qm_scr[p, heads, :], nt, preferred_element_type=jnp.float32
            )
            dprob = lax.dot_general(
                vv_scr[p, keys, :], gm_scr[p, heads, :], nt, preferred_element_type=jnp.float32
            )
            return scores, dprob

        def weigh(p, h, scores, dprob):
            tok = slice(p * QB, (p + 1) * QB)
            log2 = jnp.concatenate(
                [log_ref[2 * pair : 2 * pair + 1, tok], log_ref[2 * pair + 1 : 2 * pair + 2, tok]], axis=1
            )
            log2 = log2 * LOG2E
            parts = []
            for i in range(rows // KB):
                e = h * (rows // KB) + i
                penalty = jnp.where(table_ref[NSEL + e, p] >= 0, jnp.float32(0.0), jnp.float32(DEAD))
                part = scores[i * KB : (i + 1) * KB] * LOG2E - (log2 + penalty)
                if e < diagonal:
                    part = jnp.where(causal[e * KB : (e + 1) * KB], part, -DEAD)
                parts.append(part)
            prob = jnp.exp2(jnp.concatenate(parts, axis=0))
            prob_b = prob.astype(jnp.bfloat16)
            pb_scr[p, h * rows : (h + 1) * rows, heads] = prob_b
            seen = prob_b.astype(jnp.float32)
            delta = jnp.sum(seen * dprob, axis=0, keepdims=True)

            return prob, delta

        def finish_block(p, probs, dprobs, delta):
            tok = slice(p * QB, (p + 1) * QB)
            dq = None
            for h in range(1):
                keys = slice(h * rows, (h + 1) * rows)
                prob, dprob = probs[h], dprobs[h]
                dscore_b = (prob * (dprob - delta)).astype(jnp.bfloat16)
                ds_scr[p, keys, heads] = dscore_b
            dq = jnp.dot(kt_scr[p], ds_scr[p, :, heads], preferred_element_type=jnp.float32)
            dq = jnp.concatenate([dq[:, :QB], dq[:, QB:]], axis=0)
            qgt_scr[at : at + 2 * DH, tok] = dq.astype(jnp.bfloat16)
            qg_ref[tok, at : at + 2 * DH] = dq.T.astype(jnp.bfloat16)

        ready = multiply(0, 0)
        for p in range(per_dev):
            now = ready
            ready = multiply(p + 1, 0) if p + 1 < per_dev else None
            prob, delta = weigh(p, 0, *now)
            finish_block(p, [prob], [now[1]], delta)
            if p == per_dev // 2:
                advance("mid", pair)

    low_row = lax.broadcasted_iota(jnp.int32, (NSEL * KB, 2 * DH), 1) < DH

    def key_value(p):
        dk = jnp.dot(ds_scr[p], qm_scr[p], preferred_element_type=jnp.float32)
        dv = jnp.dot(pb_scr[p], gm_scr[p], preferred_element_type=jnp.float32)
        near = jnp.where(low_row, dk, dv)
        far = jnp.where(low_row, dv, dk)
        dkv = near + pltpu.roll(far, DH, 1)
        dkv_scr[p * NSEL : (p + 1) * NSEL] = dkv.reshape(NSEL, KB, 2 * DH)

    def product(pair):
        cols = slice(pair * GROUP * 2 * DH, (pair + 1) * GROUP * 2 * DH)

        def piece(j, carry):
            at = pl.multiple_of(j * 2 * rows, 2 * rows)
            part = jnp.dot(
                qgt_scr[cols, :], in_scr[:, pl.ds(at, 2 * rows)], preferred_element_type=jnp.float32
            )
            total[2 * j, cols, :] = part[:, :rows]
            total[2 * j + 1, cols, :] = part[:, rows:]
            return carry

        lax.fori_loop(0, kv_count // 2, piece, 0, unroll=PIECES)

    def owner_of(c, slot):
        owner = me
        for k in range(bits):
            if (slot >> (bits - 1 - k)) & 1:
                owner = flip(owner, orders[c][k])
        return owner

    def current(c, slot, k):
        at = owner_of(c, slot)
        value = total[at, c * DH : (c + 1) * DH, :]
        if k > 0:
            value = value + recv_scr[k - 1][c, slot].astype(jnp.float32)
            total[at, c * DH : (c + 1) * DH, :] = value
        return value

    def weight_copy(c, k):
        return pltpu.make_async_remote_copy(
            src_ref=send_scr[k].at[c],
            dst_ref=recv_scr[k].at[c],
            send_sem=w_send.at[c],
            recv_sem=w_recv.at[c, k],
            device_id=(flip(me, orders[c][k]), core),
            device_id_type=MESH,
        )

    def place(c, value):
        wg_ref[:, c * DH : (c + 1) * DH] = value.T

    def weight_stage(pair, k):
        left = kv_count >> (k + 1)
        for c in range(2 * GROUP * pair, 2 * GROUP * (pair + 1)):
            if k > 0:
                weight_copy(c, k - 1).wait_recv()
                weight_copy(c, k - 1).wait_send()
            if k == bits:
                value = total[me, c * DH : (c + 1) * DH, :] + recv_scr[k - 1][c, 0].astype(jnp.float32)
                place(c, value)
                continue
            for slot in range(left, 2 * left):
                send_scr[k][c, slot - left] = current(c, slot, k).astype(jnp.bfloat16)
            weight_copy(c, k).start()
            if k > 0:
                for slot in range(left):
                    current(c, slot, k)

    def advance(*point):
        for pair, k in chosen.get(point, ()):
            weight_stage(pair, k)

    tp_copy = pltpu.make_async_remote_copy(
        src_ref=half_scr.at[other],
        dst_ref=tp_scr,
        send_sem=tp_send,
        recv_sem=tp_recv,
        device_id=(me, other),
        device_id_type=MESH,
    )

    ret_start, ret_every = exchange(slot_scr, ret_scr, (ret_send, ret_recv))

    def collect(s, carry):
        value = dkv_scr[table_ref[2 * NSEL + s, 0]]
        for p in range(1, per_dev):
            value = value + dkv_scr[table_ref[2 * NSEL + s, p]]
        half_scr[0, s] = value[:half]
        half_scr[1, s] = value[half:]
        return carry

    chosen, sends, finals = plan(pair_count, per_dev, bits)
    for pair in range(pair_count):
        attend(pair)
        if pair == 0:
            loads[5].wait()
        product(pair)
        advance("end", pair)
    for p in range(per_dev):
        key_value(p)
        advance("key", p)
    lax.fori_loop(0, slot_count, collect, 0)
    for p in range(per_dev):
        at = slot_count + p * diagonal
        half_scr[0, at : at + diagonal] = dkv_scr[p * NSEL : p * NSEL + diagonal, :half, :]
        half_scr[1, at : at + diagonal] = dkv_scr[p * NSEL : p * NSEL + diagonal, half:, :]
    tp_copy.start()
    for ready, pair, k in sends:
        if ready < TP_US:
            weight_stage(pair, k)

    tp_copy.wait_recv()
    mine = half_scr.at[core]
    slot_scr[...] = (
        (mine[:slot_count] + tp_scr[:slot_count])
        .astype(jnp.bfloat16)
        .reshape(kv_count, CAP, half, 2 * DH)
    )
    ret_start()
    own_sum = (mine[slot_count:] + tp_scr[slot_count:]).reshape(own_blocks * half, 2 * DH)

    for ready, pair, k in sends:
        if ready >= TP_US:
            weight_stage(pair, k)
    for ready, pair, k in finals[:-1]:
        weight_stage(pair, k)
    ret_every.wait_recv()
    column = lax.broadcasted_iota(jnp.int32, (1, slot_count * half), 1)
    block = jnp.zeros(column.shape, jnp.int32)
    for r in range(kv_count):
        for s in range(CAP):
            block = jnp.where(column // half == r * CAP + s, first_ref[s, r * per_dev], block)
    wanted = block * half + column % half
    row = lax.broadcasted_iota(jnp.int32, (own_blocks * half, slot_count * half), 0)
    spread = jnp.where(row == wanted, 1.0, 0.0).astype(jnp.bfloat16)
    back = ret_scr[...].reshape(slot_count * half, 2 * DH)
    kvg = own_sum + jnp.dot(spread, back, preferred_element_type=jnp.float32)
    kvg_ref[...] = kvg.reshape(own_blocks, half, 2 * DH)
    get_every.wait_send()
    ret_every.wait_send()
    tp_copy.wait_send()
    for ready, pair, k in finals[-1:]:
        weight_stage(pair, k)


def padded(chosen):
    fill = jnp.full((NSEL, 128 - chosen.shape[1]), -1, jnp.int32)
    return jnp.concatenate([chosen, fill], axis=1)


def first_table(chosen, base, own_blocks, per_dev):
    inside = (chosen >= base) & (chosen < base + own_blocks)
    low = jnp.min(jnp.where(inside, chosen - base, own_blocks), axis=0, keepdims=True)
    high = jnp.max(jnp.where(inside, chosen - base, -1), axis=0, keepdims=True)
    cover = 1
    while cover < per_dev:
        shift = 128 - min(cover, per_dev - cover)
        low = jnp.minimum(low, pltpu.roll(low, shift, 1))
        high = jnp.maximum(high, pltpu.roll(high, shift, 1))
        cover = min(2 * cover, per_dev)
    low = jnp.where(low == own_blocks, 0, low)
    high = jnp.maximum(high, 0)
    row = lax.broadcasted_iota(jnp.int32, (8, 128), 0)
    return jnp.where(row == 0, low, high)


def entry_table(chosen, me, kv_count, own_blocks, per_dev):
    slot_count = kv_count * CAP
    spare = per_dev * NSEL
    lane = lax.broadcasted_iota(jnp.int32, (NSEL, 128), 1)
    entry = lax.broadcasted_iota(jnp.int32, (NSEL, 128), 0) + lane * NSEL
    blocks = pltpu.roll(chosen, lax.rem(128 - me * per_dev + 128, 128), 1)
    blocks = jnp.where(lane < per_dev, blocks, -1)
    top = kv_count * own_blocks
    lows = []
    for o in range(kv_count):
        inside = (blocks >= o * own_blocks) & (blocks < (o + 1) * own_blocks)
        lows.append(jnp.min(jnp.where(inside, blocks, top), axis=0, keepdims=True))
    low = jnp.min(jnp.concatenate(lows, axis=0), axis=1, keepdims=True)
    slot = jnp.full((NSEL, 128), slot_count, jnp.int32)
    for o in range(kv_count):
        inside = (blocks >= o * own_blocks) & (blocks < (o + 1) * own_blocks)
        at = o * CAP + jnp.where(blocks > low[o : o + 1], 1, 0)
        slot = jnp.where(inside, at, slot)
    mine = (blocks >= me * own_blocks) & (blocks < (me + 1) * own_blocks)
    slot = jnp.where(mine, slot_count, slot)
    places = []
    for s in range(slot_count):
        found = jnp.max(jnp.where(slot == s, entry, -1), axis=0, keepdims=True)
        places.append(jnp.where(found < 0, spare, found))
    used = jnp.minimum(slot, slot_count - 1)
    return jnp.concatenate([used // CAP, blocks] + places + [used % CAP], axis=0)


def finish_kernel(qg_ref, wg_ref, kvg_ref, qg_out, wg_out, kvg_out, sem):
    pairs = ((qg_ref, qg_out), (wg_ref, wg_out), (kvg_ref, kvg_out))
    copies = [pltpu.make_async_copy(src, dst, sem.at[i]) for i, (src, dst) in enumerate(pairs)]
    for copy in copies:
        copy.start()
    for copy in copies:
        copy.wait()


def finish(*results):
    hbm = pl.BlockSpec(memory_space=pl.ANY)
    return pl.pallas_call(
        finish_kernel,
        out_shape=[jax.ShapeDtypeStruct(r.shape, r.dtype) for r in results],
        in_specs=[hbm] * 3,
        out_specs=[hbm] * 3,
        scratch_shapes=[pltpu.SemaphoreType.DMA((3,))],
        compiler_params=pltpu.CompilerParams(vmem_limit_bytes=1024 * 1024),
        name="finish",
    )(*results)


def fused(kv_count, chosen, own_kv, log_sums, queries, out_grad, inputs):
    operands = (chosen, own_kv, log_sums, queries, out_grad, inputs)
    tok_count, width = queries.shape
    per_dev = tok_count // QB
    rows = inputs.shape[1] // kv_count
    chunk_count = width // DH
    orders = bit_orders(kv_count, chunk_count)
    bits = len(orders[0])
    slot_count = kv_count * CAP
    pool_count = slot_count + own_kv.shape[0]
    half = KB // 2
    parts = [
        pltpu.VMEM((chunk_count, kv_count >> (k + 1), DH, rows), jnp.bfloat16) for k in range(bits)
    ]
    vmem = pl.BlockSpec(memory_space=pltpu.VMEM)
    hbm = pl.BlockSpec(memory_space=pl.ANY)
    dma = pltpu.SemaphoreType.DMA
    table_rows = 3 * NSEL + slot_count
    return pl.pallas_call(
        functools.partial(fused_kernel, kv_count, orders),
        out_shape=[
            pltpu.VMEM((tok_count, width), jnp.bfloat16),
            pltpu.VMEM((rows, width), jnp.float32),
            pltpu.VMEM((own_kv.shape[0], half, 2 * DH), jnp.float32),
        ],
        in_specs=[hbm] * 6,
        out_specs=[vmem] * 3,
        scratch_shapes=[
            pltpu.VMEM(chosen.shape, jnp.int32),
            pltpu.VMEM((8, 128), jnp.int32),
            pltpu.VMEM((table_rows, 128), jnp.int32),
            pltpu.SMEM((8, 128), jnp.int32),
            pltpu.SMEM((table_rows, 128), jnp.int32),
            pltpu.VMEM((kv_count, CAP, KB, 2 * DH), jnp.bfloat16),
            pltpu.VMEM(log_sums.shape, jnp.float32),
            pltpu.VMEM(own_kv.shape, jnp.bfloat16),
            pltpu.VMEM((tok_count, width), jnp.bfloat16),
            pltpu.VMEM((tok_count, width), jnp.bfloat16),
            pltpu.VMEM(inputs.shape, jnp.bfloat16),
            pltpu.VMEM((kv_count, CAP, KB, 2 * DH), jnp.bfloat16),
            pltpu.VMEM((per_dev, NSEL * KB, 2 * DH), jnp.bfloat16),
            pltpu.VMEM((per_dev, NSEL * KB, 2 * DH), jnp.bfloat16),
            pltpu.VMEM((per_dev, DH, NSEL * KB), jnp.bfloat16),
            pltpu.VMEM((per_dev, QB * width // DH, 2 * DH), jnp.bfloat16),
            pltpu.VMEM((per_dev, QB * width // DH, 2 * DH), jnp.bfloat16),
            pltpu.VMEM((per_dev, NSEL * KB, QB * width // DH), jnp.bfloat16),
            pltpu.VMEM((per_dev, NSEL * KB, QB * width // DH), jnp.bfloat16),
            pltpu.VMEM((per_dev * NSEL + 1, KB, 2 * DH), jnp.float32),
            pltpu.VMEM((width, tok_count), jnp.bfloat16),
            pltpu.VMEM((kv_count, width, rows), jnp.float32),
            pltpu.VMEM((2, pool_count, half, 2 * DH), jnp.float32),
            pltpu.VMEM((pool_count, half, 2 * DH), jnp.float32),
            pltpu.VMEM((kv_count, CAP, half, 2 * DH), jnp.bfloat16),
            pltpu.VMEM((kv_count, CAP, half, 2 * DH), jnp.bfloat16),
        ]
        + parts
        + parts
        + [
            dma((8,)),
            dma,
            dma,
            dma,
            dma,
            dma,
            dma,
            dma((chunk_count,)),
            dma((chunk_count, bits)),
        ],
        compiler_params=pltpu.CompilerParams(
            collective_id=0, has_side_effects=True, vmem_limit_bytes=VMEM_LIMIT
        ),
        name="fused",
    )(*(pltpu.with_memory_space_constraint(x, pltpu.HBM) for x in operands))


def fused_body(queries, keyvals, log_sums, out_grad, inputs, selection):
    kv_count = lax.axis_size("kv")
    own_blocks = queries.shape[0] // KB
    own_kv = keyvals.reshape(own_blocks, KB, 2 * DH)
    results = fused(kv_count, selection.T, own_kv, log_sums, queries, out_grad, inputs)
    query_grad, weight_grad, keyval_grad = finish(*results)
    return (query_grad, keyval_grad, weight_grad)


def fits(kv_count, tp_count, tok_count, rows, width):
    power = kv_count & (kv_count - 1) == 0 and kv_count >= 8
    lanes = power and kv_count <= NSEL and kv_count * (tok_count // QB) <= 128
    return tp_count == 2 and lanes and rows % 128 == 0 and width % (2 * DH * GROUP) == 0


def step(queries, keyvals, log_sums, out_grad, inputs, selection):
    kv_count, tp_count = lax.axis_size("kv"), lax.axis_size("tp")
    chosen = fits(kv_count, tp_count, queries.shape[0], inputs.shape[1] // kv_count, queries.shape[1])
    return (fused_body if chosen else body)(
        queries, keyvals, log_sums, out_grad, inputs, selection
    )


def solution(mesh):
    return jax.shard_map(
        step,
        mesh=mesh,
        in_specs=(P("kv", "tp"), P("kv", None), P("tp", "kv"), P("kv", "tp"), P("kv", None), P()),
        out_specs=(P("kv", "tp"), P("kv", "tp", None), P("kv", "tp")),
        check_vma=False,
    )
```

```python
import functools

import jax
import jax.numpy as jnp
from jax import lax
from jax.experimental import pallas as pl
from jax.experimental.pallas import tpu as pltpu
from jax.sharding import PartitionSpec as P

DH = 64
QB = 128
KB = 32
NSEL = 16
CAP = 2
LOG2E = 1.4426950408889634
DEAD = 1e30
GROUP = 1
UNROLL = True
PIECES = 8
HOP_US = (5.5, 4.0, 3.5, 4.0)
LAST_US = (5.5, 4.0, 3.5, 4.0)
PAIR_US = 2.6
KEY_US = 0.78
TP_US = 7.4
KEYS = 7
VMEM_LIMIT = 56 * 1024 * 1024
MESH = pl.DeviceIdType.MESH


def slot_table(wanted):
    slot_rank = jnp.cumsum(wanted.astype(jnp.int32), axis=1) - 1
    return wanted[:, None, :] & (
        slot_rank[:, None, :] == jnp.arange(CAP, dtype=jnp.int32)[None, :, None]
    )


def weight_term(inputs, query_grad):
    return lax.dot_general(
        inputs, query_grad, (((0,), (0,)), ((), ())), preferred_element_type=jnp.float32
    )


def body(queries, keyvals, log_sums, out_grad, inputs, selection):
    kv_count = lax.axis_size("kv")
    own_index = lax.axis_index("kv")
    tok_count, width = queries.shape
    head_count = width // DH
    per_dev = tok_count // QB
    own_blocks = tok_count // KB
    slot_count = kv_count * CAP
    score_scale = DH ** (-0.5)
    own_kv = keyvals.reshape(own_blocks, KB, 2 * DH)
    lists = selection.reshape(kv_count, per_dev * NSEL)
    device_ids = jnp.arange(kv_count, dtype=jnp.int32)
    mine = own_index * own_blocks + jnp.arange(own_blocks, dtype=jnp.int32)
    wanted = jnp.any(lists[:, :, None] == mine[None, None, :], axis=1) & (
        device_ids[:, None] != own_index
    )
    owner_slots = slot_table(wanted)
    outgoing = jnp.einsum(
        "rsb,bkc->rskc",
        owner_slots.astype(jnp.bfloat16),
        own_kv,
        preferred_element_type=jnp.float32,
    ).astype(jnp.bfloat16)
    fetched = lax.all_to_all(outgoing, "kv", split_axis=0, concat_axis=0, tiled=True)
    block_list = lax.dynamic_index_in_dim(lists, own_index, 0, keepdims=False)
    every_block = jnp.arange(kv_count * own_blocks, dtype=jnp.int32)
    hits = block_list[:, None] == every_block[None, :]
    needed = jnp.any(hits, axis=0).reshape(kv_count, own_blocks) & (
        device_ids[:, None] != own_index
    )
    slot_rank = jnp.cumsum(needed.astype(jnp.int32), axis=1) - 1
    entry_rank = jnp.sum(jnp.where(hits, slot_rank.reshape(-1)[None, :], 0), axis=1)
    safe_list = jnp.maximum(block_list, 0)
    owner_index = safe_list // own_blocks
    local_block = safe_list % own_blocks
    pool_index = jnp.where(
        owner_index == own_index, slot_count + local_block, owner_index * CAP + entry_rank
    )
    pool_index = jnp.where(block_list < 0, 0, pool_index)
    block_pool = jnp.concatenate([fetched.reshape(slot_count, KB, 2 * DH), own_kv], axis=0)
    gathered = jnp.take(block_pool, pool_index, axis=0).reshape(per_dev, NSEL * KB, 2 * DH)
    key_rows = gathered[:, :, :DH]
    value_rows = gathered[:, :, DH:]
    query_rows = queries.reshape(per_dev, QB, head_count, DH)
    grad_rows = out_grad.reshape(per_dev, QB, head_count, DH)
    log_rows = log_sums.reshape(head_count, per_dev, QB).transpose(1, 0, 2)
    key_pos = (
        safe_list.reshape(per_dev, NSEL, 1) * KB + jnp.arange(KB, dtype=jnp.int32)[None, None, :]
    ).reshape(per_dev, NSEL * KB)
    key_live = jnp.repeat((block_list >= 0).reshape(per_dev, NSEL), KB, axis=1)
    query_pos = own_index * tok_count + jnp.arange(tok_count, dtype=jnp.int32).reshape(per_dev, QB)
    live_mask = key_live[:, None, :] & (key_pos[:, None, :] <= query_pos[:, :, None])
    scores = (
        jnp.einsum("pthd,pkd->phtk", query_rows, key_rows, preferred_element_type=jnp.float32)
        * score_scale
    )
    prob_f32 = jnp.where(live_mask[:, None], jnp.exp(scores - log_rows[..., None]), 0.0)
    prob_b = prob_f32.astype(jnp.bfloat16)
    recomputed = jnp.einsum(
        "phtk,pkd->pthd", prob_b, value_rows, preferred_element_type=jnp.float32
    )
    row_delta = jnp.sum(grad_rows.astype(jnp.float32) * recomputed, axis=-1)
    dprob = jnp.einsum("pthd,pkd->phtk", grad_rows, value_rows, preferred_element_type=jnp.float32)
    dscore = prob_f32 * (dprob - row_delta.transpose(0, 2, 1)[..., None])
    dscore_b = dscore.astype(jnp.bfloat16)
    query_grad = (
        (
            jnp.einsum("phtk,pkd->pthd", dscore_b, key_rows, preferred_element_type=jnp.float32)
            * score_scale
        )
        .astype(jnp.bfloat16)
        .reshape(tok_count, width)
    )
    key_grad = (
        jnp.einsum("phtk,pthd->pkd", dscore_b, query_rows, preferred_element_type=jnp.float32)
        * score_scale
    )
    value_grad = jnp.einsum("phtk,pthd->pkd", prob_b, grad_rows, preferred_element_type=jnp.float32)
    entry_grads = jnp.concatenate([key_grad, value_grad], axis=-1).reshape(
        per_dev * NSEL, KB, 2 * DH
    )
    spread = (
        pool_index[:, None] == jnp.arange(slot_count + own_blocks, dtype=jnp.int32)[None, :]
    ).astype(jnp.float32)
    shares = lax.psum_scatter(entry_grads, "tp", scatter_dimension=1, tiled=True)
    summed = jnp.einsum("ep,ekc->pkc", spread, shares, precision=lax.Precision.HIGHEST)
    key_share = summed.shape[1]
    returned = lax.all_to_all(
        summed[:slot_count].reshape(kv_count, CAP, key_share, 2 * DH).astype(jnp.bfloat16),
        "kv",
        split_axis=0,
        concat_axis=0,
        tiled=True,
    ).astype(jnp.float32)
    keyval_grad = (
        jnp.einsum(
            "rsb,rskc->bkc",
            owner_slots.astype(jnp.float32),
            returned,
            precision=lax.Precision.HIGHEST,
        )
        + summed[slot_count:]
    )
    weight_grad = lax.psum_scatter(
        weight_term(inputs, query_grad), "kv", scatter_dimension=0, tiled=True
    )
    return (query_grad, keyval_grad, weight_grad)


def bit_orders(kv_count, chunk_count):
    bits = kv_count.bit_length() - 1
    orders = []
    for c in range(chunk_count):
        turn = c % 3
        first = [0, 1, 2]
        orders.append(first[turn:] + first[:turn] + list(range(3, bits)))
    return orders


def plan(pair_count, per_dev, bits):
    points = []
    for pair in range(pair_count):
        points += [("mid", pair, PAIR_US * (pair + 0.5)), ("end", pair, PAIR_US * (pair + 1))]
    last = PAIR_US * pair_count
    points += [("key", p, last + KEY_US * (p + 1)) for p in range(per_dev)]
    chosen, sends, finals = {}, [], []
    for pair in range(pair_count):
        hops = LAST_US if pair == pair_count - 1 else HOP_US
        lags = hops[: bits - 1] + hops[-1:]
        chosen.setdefault(("end", pair), []).append((pair, 0))
        ready = PAIR_US * (pair + 1)
        for k, lag in enumerate(lags):
            ready += lag
            fitting = [point for point in points if point[2] >= ready]
            if fitting and k + 1 < len(lags):
                chosen.setdefault(fitting[0][:2], []).append((pair, k + 1))
                ready = fitting[0][2]
            elif k + 1 < len(lags):
                sends.append((ready - last, pair, k + 1))
            else:
                finals.append((ready - last, pair, k + 1))
    return chosen, sorted(sends), finals


def flip(index, place):
    bit = (index // (1 << place)) % 2
    return index + (1 - 2 * bit) * (1 << place)


def fused_kernel(
    kv_count,
    orders,
    sel_hbm,
    own_hbm,
    log_hbm,
    q_hbm,
    g_hbm,
    in_hbm,
    qg_ref,
    wg_ref,
    kvg_ref,
    sel_scr,
    first_scr,
    table_scr,
    first_ref,
    table_ref,
    out_scr,
    log_ref,
    own_scr,
    q_scr,
    g_scr,
    in_scr,
    pool_scr,
    kk_scr,
    vv_scr,
    kt_scr,
    qm_scr,
    gm_scr,
    ds_scr,
    pb_scr,
    near_prob,
    near_dprob,
    near_delta,
    dkv_scr,
    qgt_scr,
    total,
    half_scr,
    tp_scr,
    slot_scr,
    ret_scr,
    *rest,
):
    bits = len(orders[0])
    chunk_count = len(orders)
    send_scr = rest[:bits]
    recv_scr = rest[bits : 2 * bits]
    load_sem, get_send, get_recv, tp_send, tp_recv, ret_send, ret_recv, w_send, w_recv = rest[2 * bits :]
    me = lax.axis_index("kv")
    core = lax.axis_index("tp")
    other = 1 - core
    rows, width = wg_ref.shape
    pair_count = width // (2 * DH * GROUP)
    per_dev = q_scr.shape[0] // QB
    slot_count = kv_count * CAP
    entry_count = per_dev * NSEL
    diagonal = QB // KB
    half = KB // 2
    score_scale = DH ** (-0.5)

    def peer(step):
        return lax.rem(me + step, kv_count)

    own_blocks = own_hbm.shape[0]
    loads = [
        pltpu.make_async_copy(src, dst, load_sem.at[i])
        for i, (src, dst) in enumerate(
            (
                (sel_hbm, sel_scr),
                (own_hbm, own_scr),
                (log_hbm, log_ref),
                (q_hbm, q_scr),
                (g_hbm, g_scr),
                (in_hbm, in_scr),
                (first_scr, first_ref),
                (table_scr, table_ref),
            )
        )
    ]
    for load in loads[:6]:
        load.start()
    pool_scr[me] = jnp.zeros(pool_scr.shape[1:], jnp.bfloat16)
    ret_scr[me] = jnp.zeros(ret_scr.shape[1:], jnp.bfloat16)

    barrier = pltpu.get_barrier_semaphore()
    for step in range(1, kv_count):
        pl.semaphore_signal(barrier, inc=1, device_id=(peer(step), core), device_id_type=MESH)
    pl.semaphore_signal(barrier, inc=1, device_id=(me, other), device_id_type=MESH)

    loads[0].wait()
    chosen = padded(sel_scr[...])
    first_scr[...] = first_table(chosen, me * own_blocks, own_blocks, per_dev)
    loads[6].start()
    table_scr[...] = entry_table(chosen, me, kv_count, own_blocks, per_dev)
    loads[7].start()
    dkv_scr[entry_count] = jnp.zeros((KB, 2 * DH), jnp.float32)
    loads[1].wait()
    loads[6].wait()
    for r in range(kv_count):
        for s in range(CAP):
            out_scr[r, s] = own_scr[first_ref[s, r * per_dev]]
    pl.semaphore_wait(barrier, kv_count)

    def exchange(send, receive, sems):
        def copy(src_ref, dst_ref, target):
            return pltpu.make_async_remote_copy(
                src_ref=src_ref,
                dst_ref=dst_ref,
                send_sem=sems[0],
                recv_sem=sems[1],
                device_id=(target, core),
                device_id_type=MESH,
            )

        def start():
            for step in range(kv_count - 1, 0, -1):
                copy(send.at[peer(step)], receive.at[me], peer(step)).start()

        every = copy(send.at[: kv_count - 1], receive.at[: kv_count - 1], peer(1))
        return start, every

    get_start, get_every = exchange(out_scr, pool_scr, (get_send, get_recv))
    get_start()
    for load in loads[2:5]:
        load.wait()
    low_half = lax.broadcasted_iota(jnp.int32, (QB, 2 * DH), 1) < DH

    def prepare(p, carry):
        tok = pl.ds(pl.multiple_of(p * QB, QB), QB)
        for pair in range(pair_count):
            cols = slice(pair * 2 * DH, (pair + 1) * 2 * DH)
            for src, dst, scale in ((q_scr, qm_scr, score_scale), (g_scr, gm_scr, 1.0)):
                both = src[tok, cols] * jnp.asarray(scale, jnp.bfloat16)
                zero = jnp.zeros_like(both)
                at = pair * 2 * QB
                dst[p, at : at + QB, :] = jnp.where(low_half, both, zero)
                dst[p, at + QB : at + 2 * QB, :] = jnp.where(low_half, zero, both)
        return carry

    lax.fori_loop(0, per_dev, prepare, 0)
    low_key = lax.broadcasted_iota(jnp.int32, (KB, 2 * DH), 1) < DH
    key_scale = jnp.asarray(score_scale, jnp.bfloat16)

    def spread_block(p, e, both):
        rows = slice(e * KB, (e + 1) * KB)
        turned = jnp.concatenate([both[:, DH:], both[:, :DH]], axis=1)
        kk_scr[p, rows, :] = jnp.where(low_key, both, turned)
        vv_scr[p, rows, :] = jnp.where(low_key, turned, both)

    for p in range(per_dev):
        for e in range(diagonal):
            spread_block(p, e, own_scr[p * diagonal + e])
        kt_scr[p, :, :QB] = kk_scr[p, :QB, :DH].T * key_scale
    key_row = lax.broadcasted_iota(jnp.int32, (QB, 2 * QB), 0)
    query_col = lax.broadcasted_iota(jnp.int32, (QB, 2 * QB), 1) % QB
    causal = key_row <= query_col
    nt = (((1,), (1,)), ((), ()))

    def multiply(p, pair, first, last):
        heads = slice(pair * 2 * QB, (pair + 1) * 2 * QB)
        scores = lax.dot_general(
            kk_scr[p, first:last, :], qm_scr[p, heads, :], nt, preferred_element_type=jnp.float32
        )
        dprob = lax.dot_general(
            vv_scr[p, first:last, :], gm_scr[p, heads, :], nt, preferred_element_type=jnp.float32
        )
        return scores, dprob

    def weigh(p, pair, first, last, scores, dprob):
        tok = slice(p * QB, (p + 1) * QB)
        heads = slice(pair * 2 * QB, (pair + 1) * 2 * QB)
        log2 = jnp.concatenate(
            [log_ref[2 * pair : 2 * pair + 1, tok], log_ref[2 * pair + 1 : 2 * pair + 2, tok]], axis=1
        )
        log2 = log2 * LOG2E
        parts = []
        for e in range(first, last):
            part = scores[(e - first) * KB : (e - first + 1) * KB] * LOG2E
            if e < diagonal:
                part = jnp.where(causal[e * KB : (e + 1) * KB], part - log2, -DEAD)
            else:
                penalty = jnp.where(table_ref[NSEL + e, p] >= 0, jnp.float32(0.0), jnp.float32(DEAD))
                part = part - (log2 + penalty)
            parts.append(part)
        prob = jnp.exp2(jnp.concatenate(parts, axis=0))
        prob_b = prob.astype(jnp.bfloat16)
        pb_scr[p, first * KB : last * KB, heads] = prob_b
        delta = jnp.sum(prob_b.astype(jnp.float32) * dprob, axis=0, keepdims=True)
        return prob, delta

    steps = [(p, pair) for p in range(per_dev) for pair in range(pair_count)]
    ready = multiply(*steps[0], 0, QB)
    for i, (p, pair) in enumerate(steps):
        now = ready
        ready = multiply(*steps[i + 1], 0, QB) if i + 1 < len(steps) else None
        prob, delta = weigh(p, pair, 0, diagonal, *now)
        near_prob[i] = prob
        near_dprob[i] = now[1]
        near_delta[i] = jnp.broadcast_to(delta, near_delta.shape[1:])
    loads[7].wait()
    get_every.wait_recv()
    for p in range(per_dev):
        for e in range(diagonal, NSEL):
            spread_block(p, e, pool_scr[table_ref[e, p], table_ref[2 * NSEL + slot_count + e, p]])
        kt_scr[p, :, QB:] = kk_scr[p, QB:, :DH].T * key_scale

    def attend(pair):
        at = pair * 2 * DH
        heads = slice(pair * 2 * QB, (pair + 1) * 2 * QB)

        def finish_block(p, prob, dprob, delta):
            tok = slice(p * QB, (p + 1) * QB)
            slot = p * pair_count + pair
            delta = delta + near_delta[slot][:1]
            near = near_prob[slot] * (near_dprob[slot] - delta)
            far = prob * (dprob - delta)
            dscore_b = jnp.concatenate([near, far], axis=0).astype(jnp.bfloat16)
            ds_scr[p, :, heads] = dscore_b
            dq = jnp.dot(kt_scr[p], dscore_b, preferred_element_type=jnp.float32)
            dq = jnp.concatenate([dq[:, :QB], dq[:, QB:]], axis=0)
            qgt_scr[at : at + 2 * DH, tok] = dq.astype(jnp.bfloat16)
            qg_ref[tok, at : at + 2 * DH] = dq.T.astype(jnp.bfloat16)

        ready = multiply(0, pair, QB, NSEL * KB)
        for p in range(per_dev):
            now = ready
            ready = multiply(p + 1, pair, QB, NSEL * KB) if p + 1 < per_dev else None
            prob, delta = weigh(p, pair, diagonal, NSEL, *now)
            finish_block(p, prob, now[1], delta)
            if p == per_dev // 2:
                advance("mid", pair)

    low_row = lax.broadcasted_iota(jnp.int32, (NSEL * KB, 2 * DH), 1) < DH

    def key_value(p):
        dk = jnp.dot(ds_scr[p], qm_scr[p], preferred_element_type=jnp.float32)
        dv = jnp.dot(pb_scr[p], gm_scr[p], preferred_element_type=jnp.float32)
        near = jnp.where(low_row, dk, dv)
        far = jnp.where(low_row, dv, dk)
        dkv = near + pltpu.roll(far, DH, 1)
        dkv_scr[p * NSEL : (p + 1) * NSEL] = dkv.reshape(NSEL, KB, 2 * DH)

    def product(pair):
        cols = slice(pair * GROUP * 2 * DH, (pair + 1) * GROUP * 2 * DH)

        def piece(j, carry):
            at = pl.multiple_of(j * 2 * rows, 2 * rows)
            part = jnp.dot(
                qgt_scr[cols, :], in_scr[:, pl.ds(at, 2 * rows)], preferred_element_type=jnp.float32
            )
            total[2 * j, cols, :] = part[:, :rows]
            total[2 * j + 1, cols, :] = part[:, rows:]
            return carry

        lax.fori_loop(0, kv_count // 2, piece, 0, unroll=PIECES)

    def owner_of(c, slot):
        owner = me
        for k in range(bits):
            if (slot >> (bits - 1 - k)) & 1:
                owner = flip(owner, orders[c][k])
        return owner

    def current(c, slot, k):
        at = owner_of(c, slot)
        value = total[at, c * DH : (c + 1) * DH, :]
        if k > 0:
            value = value + recv_scr[k - 1][c, slot].astype(jnp.float32)
            total[at, c * DH : (c + 1) * DH, :] = value
        return value

    def weight_copy(c, k):
        return pltpu.make_async_remote_copy(
            src_ref=send_scr[k].at[c],
            dst_ref=recv_scr[k].at[c],
            send_sem=w_send.at[c],
            recv_sem=w_recv.at[c, k],
            device_id=(flip(me, orders[c][k]), core),
            device_id_type=MESH,
        )

    def place(c, value):
        wg_ref[:, c * DH : (c + 1) * DH] = value.T

    def weight_stage(pair, k):
        left = kv_count >> (k + 1)
        for c in range(2 * GROUP * pair, 2 * GROUP * (pair + 1)):
            if k > 0:
                weight_copy(c, k - 1).wait_recv()
                weight_copy(c, k - 1).wait_send()
            if k == bits:
                value = total[me, c * DH : (c + 1) * DH, :] + recv_scr[k - 1][c, 0].astype(jnp.float32)
                place(c, value)
                continue
            for slot in range(left, 2 * left):
                send_scr[k][c, slot - left] = current(c, slot, k).astype(jnp.bfloat16)
            weight_copy(c, k).start()
            if k > 0:
                for slot in range(left):
                    current(c, slot, k)

    def advance(*point):
        for pair, k in chosen.get(point, ()):
            weight_stage(pair, k)

    tp_copy = pltpu.make_async_remote_copy(
        src_ref=half_scr.at[other],
        dst_ref=tp_scr,
        send_sem=tp_send,
        recv_sem=tp_recv,
        device_id=(me, other),
        device_id_type=MESH,
    )

    ret_start, ret_every = exchange(slot_scr, ret_scr, (ret_send, ret_recv))

    def collect(s, carry):
        value = dkv_scr[table_ref[2 * NSEL + s, 0]]
        for p in range(1, per_dev):
            value = value + dkv_scr[table_ref[2 * NSEL + s, p]]
        half_scr[0, s] = value[:half]
        half_scr[1, s] = value[half:]
        return carry

    chosen, sends, finals = plan(pair_count, per_dev, bits)
    for pair in range(pair_count):
        attend(pair)
        if pair == 0:
            loads[5].wait()
        product(pair)
        advance("end", pair)
    for p in range(per_dev):
        key_value(p)
        advance("key", p)
    lax.fori_loop(0, slot_count, collect, 0)
    for p in range(per_dev):
        at = slot_count + p * diagonal
        half_scr[0, at : at + diagonal] = dkv_scr[p * NSEL : p * NSEL + diagonal, :half, :]
        half_scr[1, at : at + diagonal] = dkv_scr[p * NSEL : p * NSEL + diagonal, half:, :]
    tp_copy.start()
    for ready, pair, k in sends:
        if ready < TP_US:
            weight_stage(pair, k)

    tp_copy.wait_recv()
    mine = half_scr.at[core]
    slot_scr[...] = (
        (mine[:slot_count] + tp_scr[:slot_count])
        .astype(jnp.bfloat16)
        .reshape(kv_count, CAP, half, 2 * DH)
    )
    ret_start()
    own_sum = (mine[slot_count:] + tp_scr[slot_count:]).reshape(own_blocks * half, 2 * DH)

    for ready, pair, k in sends:
        if ready >= TP_US:
            weight_stage(pair, k)
    for ready, pair, k in finals[:-1]:
        weight_stage(pair, k)
    ret_every.wait_recv()
    column = lax.broadcasted_iota(jnp.int32, (1, slot_count * half), 1)
    block = jnp.zeros(column.shape, jnp.int32)
    for r in range(kv_count):
        for s in range(CAP):
            block = jnp.where(column // half == r * CAP + s, first_ref[s, r * per_dev], block)
    wanted = block * half + column % half
    row = lax.broadcasted_iota(jnp.int32, (own_blocks * half, slot_count * half), 0)
    spread = jnp.where(row == wanted, 1.0, 0.0).astype(jnp.bfloat16)
    back = ret_scr[...].reshape(slot_count * half, 2 * DH)
    kvg = own_sum + jnp.dot(spread, back, preferred_element_type=jnp.float32)
    kvg_ref[...] = kvg.reshape(own_blocks, half, 2 * DH)
    get_every.wait_send()
    ret_every.wait_send()
    tp_copy.wait_send()
    for ready, pair, k in finals[-1:]:
        weight_stage(pair, k)


def padded(chosen):
    fill = jnp.full((NSEL, 128 - chosen.shape[1]), -1, jnp.int32)
    return jnp.concatenate([chosen, fill], axis=1)


def first_table(chosen, base, own_blocks, per_dev):
    inside = (chosen >= base) & (chosen < base + own_blocks)
    low = jnp.min(jnp.where(inside, chosen - base, own_blocks), axis=0, keepdims=True)
    high = jnp.max(jnp.where(inside, chosen - base, -1), axis=0, keepdims=True)
    cover = 1
    while cover < per_dev:
        shift = 128 - min(cover, per_dev - cover)
        low = jnp.minimum(low, pltpu.roll(low, shift, 1))
        high = jnp.maximum(high, pltpu.roll(high, shift, 1))
        cover = min(2 * cover, per_dev)
    low = jnp.where(low == own_blocks, 0, low)
    high = jnp.maximum(high, 0)
    row = lax.broadcasted_iota(jnp.int32, (8, 128), 0)
    return jnp.where(row == 0, low, high)


def entry_table(chosen, me, kv_count, own_blocks, per_dev):
    slot_count = kv_count * CAP
    spare = per_dev * NSEL
    lane = lax.broadcasted_iota(jnp.int32, (NSEL, 128), 1)
    entry = lax.broadcasted_iota(jnp.int32, (NSEL, 128), 0) + lane * NSEL
    blocks = pltpu.roll(chosen, lax.rem(128 - me * per_dev + 128, 128), 1)
    blocks = jnp.where(lane < per_dev, blocks, -1)
    top = kv_count * own_blocks
    lows = []
    for o in range(kv_count):
        inside = (blocks >= o * own_blocks) & (blocks < (o + 1) * own_blocks)
        lows.append(jnp.min(jnp.where(inside, blocks, top), axis=0, keepdims=True))
    low = jnp.min(jnp.concatenate(lows, axis=0), axis=1, keepdims=True)
    slot = jnp.full((NSEL, 128), slot_count, jnp.int32)
    for o in range(kv_count):
        inside = (blocks >= o * own_blocks) & (blocks < (o + 1) * own_blocks)
        at = o * CAP + jnp.where(blocks > low[o : o + 1], 1, 0)
        slot = jnp.where(inside, at, slot)
    mine = (blocks >= me * own_blocks) & (blocks < (me + 1) * own_blocks)
    slot = jnp.where(mine, slot_count, slot)
    places = []
    for s in range(slot_count):
        found = jnp.max(jnp.where(slot == s, entry, -1), axis=0, keepdims=True)
        places.append(jnp.where(found < 0, spare, found))
    used = jnp.minimum(slot, slot_count - 1)
    return jnp.concatenate([used // CAP, blocks] + places + [used % CAP], axis=0)


def finish_kernel(qg_ref, wg_ref, kvg_ref, qg_out, wg_out, kvg_out, sem):
    pairs = ((qg_ref, qg_out), (wg_ref, wg_out), (kvg_ref, kvg_out))
    copies = [pltpu.make_async_copy(src, dst, sem.at[i]) for i, (src, dst) in enumerate(pairs)]
    for copy in copies:
        copy.start()
    for copy in copies:
        copy.wait()


def finish(*results):
    hbm = pl.BlockSpec(memory_space=pl.ANY)
    return pl.pallas_call(
        finish_kernel,
        out_shape=[jax.ShapeDtypeStruct(r.shape, r.dtype) for r in results],
        in_specs=[hbm] * 3,
        out_specs=[hbm] * 3,
        scratch_shapes=[pltpu.SemaphoreType.DMA((3,))],
        compiler_params=pltpu.CompilerParams(vmem_limit_bytes=1024 * 1024),
        name="finish",
    )(*results)


def fused(kv_count, chosen, own_kv, log_sums, queries, out_grad, inputs):
    operands = (chosen, own_kv, log_sums, queries, out_grad, inputs)
    tok_count, width = queries.shape
    per_dev = tok_count // QB
    rows = inputs.shape[1] // kv_count
    chunk_count = width // DH
    orders = bit_orders(kv_count, chunk_count)
    bits = len(orders[0])
    slot_count = kv_count * CAP
    pool_count = slot_count + own_kv.shape[0]
    half = KB // 2
    parts = [
        pltpu.VMEM((chunk_count, kv_count >> (k + 1), DH, rows), jnp.bfloat16) for k in range(bits)
    ]
    vmem = pl.BlockSpec(memory_space=pltpu.VMEM)
    hbm = pl.BlockSpec(memory_space=pl.ANY)
    dma = pltpu.SemaphoreType.DMA
    table_rows = 3 * NSEL + slot_count
    return pl.pallas_call(
        functools.partial(fused_kernel, kv_count, orders),
        out_shape=[
            pltpu.VMEM((tok_count, width), jnp.bfloat16),
            pltpu.VMEM((rows, width), jnp.float32),
            pltpu.VMEM((own_kv.shape[0], half, 2 * DH), jnp.float32),
        ],
        in_specs=[hbm] * 6,
        out_specs=[vmem] * 3,
        scratch_shapes=[
            pltpu.VMEM(chosen.shape, jnp.int32),
            pltpu.VMEM((8, 128), jnp.int32),
            pltpu.VMEM((table_rows, 128), jnp.int32),
            pltpu.SMEM((8, 128), jnp.int32),
            pltpu.SMEM((table_rows, 128), jnp.int32),
            pltpu.VMEM((kv_count, CAP, KB, 2 * DH), jnp.bfloat16),
            pltpu.VMEM(log_sums.shape, jnp.float32),
            pltpu.VMEM(own_kv.shape, jnp.bfloat16),
            pltpu.VMEM((tok_count, width), jnp.bfloat16),
            pltpu.VMEM((tok_count, width), jnp.bfloat16),
            pltpu.VMEM(inputs.shape, jnp.bfloat16),
            pltpu.VMEM((kv_count, CAP, KB, 2 * DH), jnp.bfloat16),
            pltpu.VMEM((per_dev, NSEL * KB, 2 * DH), jnp.bfloat16),
            pltpu.VMEM((per_dev, NSEL * KB, 2 * DH), jnp.bfloat16),
            pltpu.VMEM((per_dev, DH, NSEL * KB), jnp.bfloat16),
            pltpu.VMEM((per_dev, QB * width // DH, 2 * DH), jnp.bfloat16),
            pltpu.VMEM((per_dev, QB * width // DH, 2 * DH), jnp.bfloat16),
            pltpu.VMEM((per_dev, NSEL * KB, QB * width // DH), jnp.bfloat16),
            pltpu.VMEM((per_dev, NSEL * KB, QB * width // DH), jnp.bfloat16),
            pltpu.VMEM((per_dev * chunk_count // 2, QB, 2 * QB), jnp.float32),
            pltpu.VMEM((per_dev * chunk_count // 2, QB, 2 * QB), jnp.float32),
            pltpu.VMEM((per_dev * chunk_count // 2, 8, 2 * QB), jnp.float32),
            pltpu.VMEM((per_dev * NSEL + 1, KB, 2 * DH), jnp.float32),
            pltpu.VMEM((width, tok_count), jnp.bfloat16),
            pltpu.VMEM((kv_count, width, rows), jnp.float32),
            pltpu.VMEM((2, pool_count, half, 2 * DH), jnp.float32),
            pltpu.VMEM((pool_count, half, 2 * DH), jnp.float32),
            pltpu.VMEM((kv_count, CAP, half, 2 * DH), jnp.bfloat16),
            pltpu.VMEM((kv_count, CAP, half, 2 * DH), jnp.bfloat16),
        ]
        + parts
        + parts
        + [
            dma((8,)),
            dma,
            dma,
            dma,
            dma,
            dma,
            dma,
            dma((chunk_count,)),
            dma((chunk_count, bits)),
        ],
        compiler_params=pltpu.CompilerParams(
            collective_id=0, has_side_effects=True, vmem_limit_bytes=VMEM_LIMIT
        ),
        name="fused",
    )(*(pltpu.with_memory_space_constraint(x, pltpu.HBM) for x in operands))


def fused_body(queries, keyvals, log_sums, out_grad, inputs, selection):
    kv_count = lax.axis_size("kv")
    own_blocks = queries.shape[0] // KB
    own_kv = keyvals.reshape(own_blocks, KB, 2 * DH)
    results = fused(kv_count, selection.T, own_kv, log_sums, queries, out_grad, inputs)
    query_grad, weight_grad, keyval_grad = finish(*results)
    return (query_grad, keyval_grad, weight_grad)


def fits(kv_count, tp_count, tok_count, rows, width):
    power = kv_count & (kv_count - 1) == 0 and kv_count >= 8
    lanes = power and kv_count <= NSEL and kv_count * (tok_count // QB) <= 128
    return tp_count == 2 and lanes and rows % 128 == 0 and width % (2 * DH * GROUP) == 0


def step(queries, keyvals, log_sums, out_grad, inputs, selection):
    kv_count, tp_count = lax.axis_size("kv"), lax.axis_size("tp")
    chosen = fits(kv_count, tp_count, queries.shape[0], inputs.shape[1] // kv_count, queries.shape[1])
    return (fused_body if chosen else body)(
        queries, keyvals, log_sums, out_grad, inputs, selection
    )


def solution(mesh):
    return jax.shard_map(
        step,
        mesh=mesh,
        in_specs=(P("kv", "tp"), P("kv", None), P("tp", "kv"), P("kv", "tp"), P("kv", None), P()),
        out_specs=(P("kv", "tp"), P("kv", "tp", None), P("kv", "tp")),
        check_vma=False,
    )
```
